512 devices in a mesh: sp: 128 (over z, y, core), tp: 4 (over x).
Axes of the slice: x: 4, y: 8, z: 8, core: 2. Of those that a mesh axis runs over, the one named last changes fastest.
Arguments:
- tokens: bfloat16 [16384, 2048], P(('sp', 'tp')), may hold values from -6 to 6
- doc_lengths: int32 [16], replicated, may hold values from 1 to 10240, 16384 in all
- query_down: bfloat16 [2048, 512], replicated, may hold values from -0.125 to 0.125
- latent_down: bfloat16 [2048, 256], replicated, may hold values from -0.125 to 0.125
- rope_down: bfloat16 [2048, 32], replicated, may hold values from -0.125 to 0.125
- query_latent_gain: float32 [512], replicated, may hold values from 0.1 to 1.9
- latent_gain: float32 [256], replicated, may hold values from 0.1 to 1.9
- query_up: bfloat16 [512, 768], P(None, 'tp'), may hold values from -0.25 to 0.25
- key_up: bfloat16 [256, 512], P(None, 'tp'), may hold values from -0.375 to 0.375
- value_up: bfloat16 [256, 512], P(None, 'tp'), may hold values from -0.375 to 0.375
- query_gain: float32 [96], replicated, may hold values from 0.5 to 15
- key_gain: float32 [96], replicated, may hold values from 0.5 to 15
- output_gain: float32 [512], replicated, may hold values from 0.1 to 1.9
- output_weight: bfloat16 [512, 2048], P(None, 'tp'), may hold values from -0.25 to 0.25
Outputs:
- layer_output: bfloat16 [16384, 2048], P('sp', 'tp')
- log_totals: float32 [8, 16384], P('tp', 'sp')
The draws below stay inside these ranges and needn't reach their ends.
Inputs may be any that keep to these rules, and one draw needn't show every extreme that they name: `doc_lengths`: the lengths sum to 16384; the longest is exactly 10240.
All inputs are finite; a program needn't handle non-finite values.
Results may differ from the reference program's by a relative error of at most 0.019.
The reference program's roundings to bfloat16 on the way count: a program that leaves them out, or rounds other values in their place, can miss the bound.
Values may be sent and summed in bfloat16 or wider, within the bound.
No kernel may reach another device: no remote copies, remote signals or barrier semaphores. Data moves between devices by JAX's collectives and lax.ppermute only.
A program may use at most 64 MiB of HBM per device.

```python
import math
import jax
import jax.numpy as jnp
import numpy as np
from jax import lax

D = 2048
QR = 512
KVR = 256
H = 8
NOPE = 64
ROPE = 32
VD = 64
NDOC = 16
SEQ = 16384


def gain_table(key, salt_value):
    gains_out = jax.random.uniform(jax.random.fold_in(key, salt_value), (NOPE + ROPE,), jnp.float32, 0.5, 1.5)
    return gains_out


def draw_query_gain(key, part):
    return gain_table(key, 101)


def draw_key_gain(key, part):
    return gain_table(key, 202)


def block_scale(key, dims, split, least, top_value):
    gain = 1.0
    for position, shards_of in split:
        draws = jax.random.uniform(jax.random.fold_in(jax.random.fold_in(key, 6), position), (shards_of,), jnp.float32, least / len(split), top_value / len(split))
        gain = gain * jnp.repeat(jnp.exp(draws), dims[position] // shards_of).reshape((-1,) + (1,) * (len(dims) - 1 - position))
    return gain


def length_profile(amount, total, most, lean):
    weights = [(1 << 20) // math.isqrt(standing ** lean) + 1 for standing in range(2, amount + 1)]
    rest, given = total - most - (amount - 1), [1] * (amount - 1)
    while rest > 0:
        candidates = [i for i in range(amount - 1) if given[i] < most]
        mass, remaining = sum([weights[i] for i in candidates]), rest
        for i in candidates:
            addition = min(most - given[i], max(1, remaining * weights[i] // mass), rest)
            given[i] = given[i] + addition
            rest = rest - addition
    return np.array([most] + given)


def uneven(own_key, amount, total, most, lean):
    if amount == 2:
        one = jax.random.randint(own_key, (), max(1, total - most), min(most, total - 1) + 1)
        return jnp.stack([one, total - one])
    tallies = jnp.asarray(length_profile(amount, total, most, lean), jnp.int32)
    pairs = (amount - 1) // 2
    giver, taker = tallies[1:1 + 2 * pairs:2], tallies[2:2 + 2 * pairs:2]
    margin = jnp.minimum(giver - 1, most - taker)
    shifted = jax.random.randint(jax.random.fold_in(own_key, 1), (pairs,), 0, 1 << 20) % (margin + 1)
    tallies = tallies.at[1:1 + 2 * pairs:2].set(giver - shifted).at[2:2 + 2 * pairs:2].set(taker + shifted)
    return tallies[jax.random.permutation(jax.random.fold_in(own_key, 2), amount)]


def normal_values(own_key, shape, scale, limit, shards=(), kind=jnp.bfloat16):
    level = block_scale(own_key, shape, shards, -0.22, 0.18) if shards else 1.0
    values = jax.random.normal(own_key, shape, jnp.float32) * scale * level
    return jnp.minimum(jnp.maximum(values, -limit), limit).astype(kind)


def setup_inputs(seed: int = 0) -> dict:
    keys = jax.random.split(jax.random.key(seed), 15)
    return {
        "tokens": normal_values(keys[0], (SEQ, D), 1.0, 6.0, ((0, 512),)),
        "doc_lengths": uneven(keys[1], NDOC, SEQ, SEQ * 5 // 8, 2).astype(jnp.int32),
        "query_down": normal_values(keys[2], (D, QR), D ** -0.5, 0.125),
        "latent_down": normal_values(keys[3], (D, KVR), D ** -0.5, 0.125),
        "rope_down": normal_values(keys[4], (D, ROPE), D ** -0.5, 0.125),
        "query_latent_gain": jnp.clip(1.0 + 0.18 * jax.random.normal(keys[5], (QR,), jnp.float32), 0.1, 1.9),
        "latent_gain": jnp.clip(1.0 + 0.18 * jax.random.normal(keys[6], (KVR,), jnp.float32), 0.1, 1.9),
        "query_up": normal_values(keys[7], (QR, H * (NOPE + ROPE)), QR ** -0.5, 0.25, ((1, 4),)),
        "key_up": normal_values(keys[8], (KVR, H * NOPE), KVR ** -0.5, 0.375, ((1, 4),)),
        "value_up": normal_values(keys[9], (KVR, H * VD), KVR ** -0.5, 0.375, ((1, 4),)),
        "query_gain": draw_query_gain(jax.random.fold_in(keys[14], 71), 0),
        "key_gain": draw_key_gain(jax.random.fold_in(keys[14], 71), 0),
        "output_gain": jnp.clip(1.0 + 0.18 * jax.random.normal(keys[12], (H * VD,), jnp.float32), 0.1, 1.9),
        "output_weight": normal_values(keys[13], (H * VD, D), (H * VD) ** -0.5, 0.25, ((1, 4),)),
    }


EPS = 1e-06
THETA = 10000.0
NEG = -1e+30

def norm_rows(matrix, scaling):
    mean_square = lax.optimization_barrier(jnp.mean(matrix * matrix, axis=-1, keepdims=True))
    return matrix * lax.rsqrt(mean_square + EPS) * scaling

def rotate(matrix, places):
    half_width = matrix.shape[-1] // 2
    inverse = THETA ** (-jnp.arange(half_width, dtype=jnp.float32) / half_width)
    angles = places.astype(jnp.float32)[:, None, None] * inverse
    cosine = jnp.cos(angles)
    sine_part = jnp.sin(angles)
    leading = matrix[..., :half_width]
    trailing = matrix[..., half_width:]
    return jnp.concatenate([leading * cosine - trailing * sine_part, trailing * cosine + leading * sine_part], axis=-1)

def doc_index(places, doc_ends):
    return lax.optimization_barrier(jnp.sum((places[:, None] >= doc_ends[None, :]).astype(jnp.int32), axis=1)).astype(jnp.int32)

def head_keys(latent_rows, rope_rows, places, key_up, value_up, key_gain):
    row_count = latent_rows.shape[0]
    head_count = key_up.shape[1] // NOPE
    plain_part = jnp.dot(latent_rows, key_up, preferred_element_type=jnp.float32).reshape(row_count, head_count, NOPE)
    shared_part = jnp.broadcast_to(rope_rows.astype(jnp.float32)[:, None, :], (row_count, head_count, ROPE))
    joined = norm_rows(jnp.concatenate([plain_part, shared_part], axis=-1), key_gain)
    key_block = jnp.concatenate([joined[..., :NOPE], rotate(joined[..., NOPE:], places)], axis=-1).astype(jnp.bfloat16)
    value_block = jnp.dot(latent_rows, value_up, preferred_element_type=jnp.float32).astype(jnp.bfloat16)
    return (key_block, value_block.reshape(row_count, head_count, VD))

def reference(tokens, doc_lengths, query_down, latent_down, rope_down, query_latent_gain, latent_gain, query_up, key_up, value_up, query_gain, key_gain, output_gain, output_weight):
    head_width = NOPE + ROPE
    query_latent = norm_rows(jnp.dot(tokens, query_down, preferred_element_type=jnp.float32), query_latent_gain).astype(jnp.bfloat16)
    key_latent = norm_rows(jnp.dot(tokens, latent_down, preferred_element_type=jnp.float32), latent_gain).astype(jnp.bfloat16)
    rope_key = jnp.dot(tokens, rope_down, preferred_element_type=jnp.float32).astype(jnp.bfloat16)
    places = jnp.arange(SEQ, dtype=jnp.int32)
    doc_ends = jnp.cumsum(doc_lengths).astype(jnp.int32)
    docs = doc_index(places, doc_ends)
    query_raw = jnp.dot(query_latent, query_up, preferred_element_type=jnp.float32).reshape(SEQ, H, head_width)
    query_raw = norm_rows(query_raw, query_gain)
    queries = jnp.concatenate([query_raw[..., :NOPE], rotate(query_raw[..., NOPE:], places)], axis=-1).astype(jnp.bfloat16)
    key_block, value_block = head_keys(key_latent, rope_key, places, key_up, value_up, key_gain)
    keys_wide = key_block.astype(jnp.float32)
    values_wide = value_block.astype(jnp.float32)
    block_rows = math.gcd(SEQ, 512)
    block_count = SEQ // block_rows
    score_scale = head_width ** (-0.5)

    def one_block(block_index):
        begin_at = (block_index * block_rows).astype(jnp.int32)
        query_part = lax.dynamic_slice_in_dim(queries, begin_at, block_rows, 0).astype(jnp.float32)
        query_docs = lax.dynamic_slice_in_dim(docs, begin_at, block_rows, 0)
        scores = jnp.einsum('qhd,khd->hqk', query_part, keys_wide) * score_scale
        allowed = (query_docs[:, None] == docs[None, :])[None]
        scores = jnp.where(allowed, scores, NEG)
        row_top = lax.optimization_barrier(jnp.max(scores, axis=-1))
        expd_part = jnp.where(allowed, jnp.exp(scores - row_top[..., None]), 0.0)
        row_total = lax.optimization_barrier(jnp.sum(expd_part, axis=-1))
        weights = lax.optimization_barrier(expd_part.astype(jnp.bfloat16)).astype(jnp.float32)
        weighted = jnp.einsum('hqk,khd->qhd', weights, values_wide)
        head_out = (weighted / jnp.transpose(row_total)[:, :, None]).astype(jnp.bfloat16)
        return (head_out, row_top + jnp.log(row_total))
    head_blocks, log_blocks = lax.map(one_block, jnp.arange(block_count, dtype=jnp.int32))
    head_out = head_blocks.reshape(SEQ, H * VD)
    log_totals = jnp.transpose(log_blocks, (1, 0, 2)).reshape(H, SEQ)
    normed = norm_rows(head_out.astype(jnp.float32), output_gain).astype(jnp.bfloat16)
    layer_output = jnp.dot(normed, output_weight, preferred_element_type=jnp.float32).astype(jnp.bfloat16)
    return (layer_output, log_totals)
```

```python
import math

import jax
import jax.numpy as jnp
from jax import lax
from jax.experimental import pallas as pl
from jax.experimental.pallas import tpu as pltpu
from jax.sharding import Mesh, PartitionSpec as P

NOPE = 64
ROPE = 32
VD = 64
HW = NOPE + ROPE
KV = HW + VD
HALF = ROPE // 2

EPS = 1e-06
THETA = 10000.0
NEG = -1e30
START = -1e29
ZS, YS, CS, XS = 8, 8, 2, 4
ROWS = 128
QB = 256
KB = 256
MSG = VD + 16
SCALE = HW ** (-0.5)
SCALE2 = SCALE * math.log2(math.e)

f32 = jnp.float32
bf16 = jnp.bfloat16


def norm_rows(matrix, scaling):
    mean_square = jnp.mean(matrix * matrix, axis=-1, keepdims=True)
    return matrix * lax.rsqrt(mean_square + EPS) * scaling


def spread(value, axes):
    count = 1
    for a in axes:
        count *= lax.axis_size(a)
    copies = jnp.broadcast_to(value, (count, *value.shape))
    return lax.all_to_all(copies, axes, split_axis=0, concat_axis=0, tiled=True)


def rotated(a, b, cosine, sine):
    return a * cosine - b * sine, b * cosine + a * sine


def kv_kernel(lat_ref, rope_ref, key_up_ref, value_up_ref, gain_ref, cos_ref, sin_ref, out_ref):
    lat = lat_ref[...]
    plain = lax.dot_general(
        key_up_ref[...], lat, (((0,), (1,)), ((), ())), preferred_element_type=f32
    )
    value = lax.dot_general(
        value_up_ref[...], lat, (((0,), (1,)), ((), ())), preferred_element_type=f32
    ).astype(bf16)
    shared = rope_ref[...].astype(f32)
    shared = jnp.transpose(jnp.concatenate([shared, jnp.zeros((ROWS, 128 - ROPE), f32)], axis=1))
    shared = shared[:ROPE]
    shared_square = jnp.sum(shared * shared, axis=0, keepdims=True)
    gain = gain_ref[...]
    cosine, sine = cos_ref[...], sin_ref[...]
    for c in range(CS):
        mine = plain[c * NOPE : (c + 1) * NOPE]
        square = (jnp.sum(mine * mine, axis=0, keepdims=True) + shared_square) * (1.0 / HW)
        scale = lax.rsqrt(square + EPS)
        top = mine * scale * gain[:NOPE]
        low = shared * scale * gain[NOPE:]
        a, b = rotated(low[:HALF], low[HALF:], cosine, sine)
        block = jnp.concatenate([top, a, b], axis=0).astype(bf16)
        for z in range(ZS):
            out_ref[z * CS + c, :HW, :] = block
            out_ref[z * CS + c, HW:, :] = value[c * VD : (c + 1) * VD]


def q_kernel(lat_ref, query_up_ref, gain_ref, cos_ref, sin_ref, out_ref):
    raw = lax.dot_general(
        query_up_ref[...], lat_ref[...], (((0,), (1,)), ((), ())), preferred_element_type=f32
    )
    gain = gain_ref[...]
    cosine, sine = cos_ref[...], sin_ref[...]
    for c in range(CS):
        mine = raw[c * HW : (c + 1) * HW]
        square = jnp.sum(mine * mine, axis=0, keepdims=True) * (1.0 / HW)
        mine = mine * lax.rsqrt(square + EPS) * gain
        a, b = rotated(mine[NOPE : NOPE + HALF], mine[NOPE + HALF :], cosine, sine)
        block = jnp.concatenate([mine[:NOPE], a, b], axis=0).astype(bf16)
        for y in range(YS):
            out_ref[y * CS + c] = block


def split_rows(value, width):
    high = value.astype(bf16).astype(f32)
    rest = value - high
    middle = rest.astype(bf16).astype(f32)
    low = rest - middle
    row = lax.broadcasted_iota(jnp.int32, (16, width), 0)
    zero = jnp.zeros((16, width), f32)
    both = jnp.where(row == 0, high, jnp.where(row == 1, middle, jnp.where(row == 2, low, zero)))
    return both.astype(bf16)


def joined_rows(rows):
    rows = rows.astype(f32)
    return (rows[0:1] + rows[1:2]) + rows[2:3]


SUB = 2


def attend_kernel(
    qlo, qhi, klo, khi, qdoc_ref, kdoc_ref, q_ref, kv_ref, out_ref, k_s, q_s, m_s, l_s, acc_s
):
    for i in range(ZS * CS):
        k_s[i * ROWS : (i + 1) * ROWS, :] = jnp.transpose(
            jnp.concatenate([kv_ref[i, :HW, :], jnp.zeros((128 - HW, ROWS), bf16)], axis=0)
        )
    for i in range(YS):
        q_s[i, :HW, :] = jnp.concatenate([q_ref[2 * i], q_ref[2 * i + 1]], axis=1)
        q_s[i, HW:, :] = jnp.zeros((128 - HW, QB), bf16)
    m_s[...] = jnp.full(m_s.shape, START, f32)
    l_s[...] = jnp.zeros(l_s.shape, f32)
    acc_s[...] = jnp.zeros(acc_s.shape, f32)

    def block(t, j, masked):
        keys = k_s[pl.ds(j * KB, KB), :]
        values = jnp.concatenate([kv_ref[2 * j, HW:, :], kv_ref[2 * j + 1, HW:, :]], axis=1)
        if masked:
            key_doc = kdoc_ref[pl.ds(j * KB, KB), :]
        for s in range(SUB):
            at = t * SUB + s
            scores = jnp.dot(keys, q_s[at], preferred_element_type=f32)
            if masked:
                scores = jnp.where(key_doc == qdoc_ref[at], scores, NEG)
            before = m_s[at]
            now = jnp.maximum(before, jnp.max(scores, axis=0, keepdims=True))
            weights = jnp.exp2((scores - now) * SCALE2)
            rescale = jnp.exp2((before - now) * SCALE2)
            m_s[at] = now
            l_s[at] = l_s[at] * rescale + jnp.sum(weights, axis=0, keepdims=True)
            acc_s[at] = acc_s[at] * rescale + jnp.dot(
                values, weights.astype(bf16), preferred_element_type=f32
            )

    def query_step(t, _):
        def key_step(j, _):
            first, last = qlo[t], qhi[t]
            least, most = klo[j], khi[j]
            touches = (least <= last) & (most >= first)
            whole = (first == last) & (least == most) & (first == least)

            @pl.when(whole)
            def _():
                block(t, j, False)

            @pl.when(touches & jnp.logical_not(whole))
            def _():
                block(t, j, True)

            return 0

        return lax.fori_loop(0, ZS, key_step, 0)

    lax.fori_loop(0, YS // SUB, query_step, 0)
    for i in range(YS):
        total = l_s[i]
        some = total > 0.0
        safe = jnp.where(some, total, 1.0)
        logs = jnp.where(some, m_s[i] * SCALE + jnp.log(safe), NEG)
        out_ref[i, :VD, :] = (acc_s[i] / safe).astype(bf16)
        out_ref[i, VD:, :] = split_rows(logs, QB)


def combine_kernel(in_ref, out_ref):
    logs = [joined_rows(in_ref[i, VD:, :]) for i in range(YS)]
    top = logs[0]
    for v in logs[1:]:
        top = jnp.maximum(top, v)
    total = jnp.zeros((1, QB), f32)
    mixed = jnp.zeros((VD, QB), f32)
    for i in range(YS):
        w = jnp.exp(logs[i] - top)
        total = total + w
        mixed = mixed + w * in_ref[i, :VD, :].astype(f32)
    head = (mixed / total).astype(bf16)
    tail = split_rows(top + jnp.log(total), QB)
    for c in range(CS):
        for x in range(XS):
            out_ref[c * XS + x, :VD, :] = head[:, c * ROWS : (c + 1) * ROWS]
            out_ref[c * XS + x, VD:, :] = tail[:, c * ROWS : (c + 1) * ROWS]


def output_kernel(x_at, in_ref, gain_ref, weight_ref, out_ref, log_ref):
    heads = []
    for x in range(XS):
        for c in range(CS):
            heads.append(in_ref[c * XS + x, :VD, :].astype(f32))
    joined = jnp.concatenate(heads, axis=0)
    square = jnp.sum(joined * joined, axis=0, keepdims=True) * (1.0 / joined.shape[0])
    normed = (joined * lax.rsqrt(square + EPS) * gain_ref[...]).astype(bf16)
    out_ref[...] = lax.dot_general(
        normed, weight_ref[...], (((0,), (0,)), ((), ())), preferred_element_type=f32
    ).astype(bf16)
    for c in range(CS):
        log_ref[c : c + 1, :] = joined_rows(in_ref[c * XS + x_at[0], VD:, :])


def smem():
    return pl.BlockSpec(memory_space=pltpu.SMEM)


def vmem():
    return pl.BlockSpec(memory_space=pltpu.VMEM)


def call(kernel, out_shape, scalars, arrays, scratch=(), name=None):
    many = isinstance(out_shape, (tuple, list))
    return pl.pallas_call(
        kernel,
        out_shape=out_shape,
        in_specs=[smem()] * len(scalars) + [vmem()] * len(arrays),
        out_specs=[vmem() for _ in out_shape] if many else vmem(),
        scratch_shapes=list(scratch),
        compiler_params=pltpu.CompilerParams(vmem_limit_bytes=32 * 1024 * 1024),
        name=name,
    )(*scalars, *arrays)


def per_device(
    tokens,
    doc_lengths,
    query_down,
    latent_down,
    rope_down,
    query_latent_gain,
    latent_gain,
    query_up,
    key_up,
    value_up,
    query_gain,
    key_gain,
    output_gain,
    output_weight,
):
    z_at, y_at, c_at, x_at = (lax.axis_index(a) for a in ("z", "y", "c", "x"))
    query_latent = norm_rows(
        jnp.dot(tokens, query_down, preferred_element_type=f32), query_latent_gain
    ).astype(bf16)
    key_latent = norm_rows(
        jnp.dot(tokens, latent_down, preferred_element_type=f32), latent_gain
    ).astype(bf16)
    rope_key = jnp.dot(tokens, rope_down, preferred_element_type=f32).astype(bf16)
    rank_q, rank_k = query_latent.shape[1], key_latent.shape[1]
    every = spread(jnp.concatenate([query_latent, key_latent, rope_key], axis=1), ("x",))
    every = every.reshape(ROWS, -1)
    query_rows = every[:, :rank_q]
    latent_rows = every[:, rank_q : rank_q + rank_k]
    rope_rows = every[:, rank_q + rank_k :]

    offset = ((z_at * YS + y_at) * CS + c_at) * ROWS
    places = offset + jnp.arange(ROWS, dtype=jnp.int32)
    inverse = THETA ** (-jnp.arange(HALF, dtype=f32) / HALF)
    angles = places.astype(f32)[None, :] * inverse[:, None]
    cosine, sine = jnp.cos(angles), jnp.sin(angles)

    doc_ends = jnp.cumsum(doc_lengths)

    def docs_at(positions):
        return jnp.sum((positions[..., None] >= doc_ends).astype(jnp.int32), axis=-1)

    span = YS * QB
    query_places = z_at * span + jnp.arange(span, dtype=jnp.int32)
    query_docs = docs_at(query_places).reshape(YS, 1, QB)
    wide = SUB * QB
    query_starts = z_at * span + jnp.arange(YS // SUB, dtype=jnp.int32) * wide
    query_low, query_high = docs_at(query_starts), docs_at(query_starts + (wide - 1))
    key_starts = jnp.arange(ZS, dtype=jnp.int32) * span + y_at * KB
    key_low, key_high = docs_at(key_starts), docs_at(key_starts + (KB - 1))
    key_places = key_starts[:, None] + jnp.arange(KB, dtype=jnp.int32)
    key_docs = docs_at(key_places).reshape(ZS * KB, 1)

    kv_out = call(
        kv_kernel,
        jax.ShapeDtypeStruct((ZS * CS, KV, ROWS), bf16),
        (),
        (latent_rows, rope_rows, key_up, value_up, key_gain[:, None], cosine, sine),
        name="kv",
    )
    kv_all = lax.all_to_all(kv_out, ("z", "c"), split_axis=0, concat_axis=0, tiled=True)
    q_out = call(
        q_kernel,
        jax.ShapeDtypeStruct((YS * CS, HW, ROWS), bf16),
        (),
        (query_rows, query_up, query_gain[:, None], cosine, sine),
        name="q",
    )
    q_all = lax.all_to_all(q_out, ("y", "c"), split_axis=0, concat_axis=0, tiled=True)

    parts = call(
        attend_kernel,
        jax.ShapeDtypeStruct((YS, MSG, QB), bf16),
        (query_low, query_high, key_low, key_high),
        (query_docs, key_docs, q_all, kv_all),
        scratch=(
            pltpu.VMEM((ZS * KB, 128), bf16),
            pltpu.VMEM((YS, 128, QB), bf16),
            pltpu.VMEM((YS, 1, QB), f32),
            pltpu.VMEM((YS, 1, QB), f32),
            pltpu.VMEM((YS, VD, QB), f32),
        ),
        name="attend",
    )
    parts = lax.all_to_all(parts, "y", split_axis=0, concat_axis=0, tiled=True)
    heads = call(
        combine_kernel, jax.ShapeDtypeStruct((CS * XS, MSG, ROWS), bf16), (), (parts,), name="mix"
    )
    heads = lax.all_to_all(heads, ("c", "x"), split_axis=0, concat_axis=0, tiled=True)
    layer_output, log_totals = call(
        output_kernel,
        (
            jax.ShapeDtypeStruct((ROWS, output_weight.shape[1]), bf16),
            jax.ShapeDtypeStruct((CS, ROWS), f32),
        ),
        (x_at.astype(jnp.int32).reshape(1),),
        (heads, output_gain[:, None], output_weight),
        name="out",
    )
    return (layer_output, log_totals)


def solution(mesh):
    fine = Mesh(mesh.devices.reshape(ZS, YS, CS, XS), ("z", "y", "c", "x"))
    sp = ("z", "y", "c")
    return jax.shard_map(
        per_device,
        mesh=fine,
        in_specs=(
            P((*sp, "x"), None),
            P(),
            P(),
            P(),
            P(),
            P(),
            P(),
            P(None, "x"),
            P(None, "x"),
            P(None, "x"),
            P(),
            P(),
            P(),
            P(None, "x"),
        ),
        out_specs=(P(sp, "x"), P("x", sp)),
        check_vma=False,
    )
```

```python
import math

import jax
import jax.numpy as jnp
from jax import lax
from jax.experimental import pallas as pl
from jax.experimental.pallas import tpu as pltpu
from jax.sharding import Mesh, PartitionSpec as P


NOPE = 64
ROPE = 32
VD = 64
HW = NOPE + ROPE
KV = HW + VD
HALF = ROPE // 2

EPS = 1e-06
THETA = 10000.0
NEG = -1e30
START = -1e29
ZS, YS, CS, XS = 8, 8, 2, 4
ROWS = 128
QB = 256
KB = 256
MSG = VD + 16
SCALE = HW ** (-0.5)
SCALE2 = SCALE * math.log2(math.e)

f32 = jnp.float32
bf16 = jnp.bfloat16


def norm_rows(matrix, scaling):
    mean_square = jnp.mean(matrix * matrix, axis=-1, keepdims=True)
    return matrix * lax.rsqrt(mean_square + EPS) * scaling


def spread(value, axes):
    count = 1
    for a in axes:
        count *= lax.axis_size(a)
    copies = jnp.broadcast_to(value, (count, *value.shape))
    return lax.all_to_all(copies, axes, split_axis=0, concat_axis=0, tiled=True)


def rotated(a, b, cosine, sine):
    return a * cosine - b * sine, b * cosine + a * sine


def kv_kernel(lat_ref, rope_ref, key_up_ref, value_up_ref, gain_ref, cos_ref, sin_ref, out_ref):
    lat = lat_ref[...]
    plain = lax.dot_general(
        key_up_ref[...], lat, (((0,), (1,)), ((), ())), preferred_element_type=f32
    )
    value = lax.dot_general(
        value_up_ref[...], lat, (((0,), (1,)), ((), ())), preferred_element_type=f32
    ).astype(bf16)
    shared = rope_ref[...].astype(f32)
    shared = jnp.transpose(jnp.concatenate([shared, jnp.zeros((ROWS, 128 - ROPE), f32)], axis=1))
    shared = shared[:ROPE]
    shared_square = jnp.sum(shared * shared, axis=0, keepdims=True)
    gain = gain_ref[...]
    cosine, sine = cos_ref[...], sin_ref[...]
    for c in range(CS):
        mine = plain[c * NOPE : (c + 1) * NOPE]
        square = (jnp.sum(mine * mine, axis=0, keepdims=True) + shared_square) * (1.0 / HW)
        scale = lax.rsqrt(square + EPS)
        top = mine * scale * gain[:NOPE]
        low = shared * scale * gain[NOPE:]
        a, b = rotated(low[:HALF], low[HALF:], cosine, sine)
        block = jnp.concatenate([top, a, b], axis=0).astype(bf16)
        for z in range(ZS):
            out_ref[z * CS + c, :HW, :] = block
            out_ref[z * CS + c, HW:, :] = value[c * VD : (c + 1) * VD]


def q_kernel(lat_ref, query_up_ref, gain_ref, cos_ref, sin_ref, out_ref):
    raw = lax.dot_general(
        query_up_ref[...], lat_ref[...], (((0,), (1,)), ((), ())), preferred_element_type=f32
    )
    gain = gain_ref[...]
    cosine, sine = cos_ref[...], sin_ref[...]
    for c in range(CS):
        mine = raw[c * HW : (c + 1) * HW]
        square = jnp.sum(mine * mine, axis=0, keepdims=True) * (1.0 / HW)
        mine = mine * lax.rsqrt(square + EPS) * gain
        a, b = rotated(mine[NOPE : NOPE + HALF], mine[NOPE + HALF :], cosine, sine)
        block = jnp.concatenate([mine[:NOPE], a, b], axis=0).astype(bf16)
        out_ref[c * HW : (c + 1) * HW, :] = block


def split_rows(value, width):
    high = value.astype(bf16).astype(f32)
    rest = value - high
    middle = rest.astype(bf16).astype(f32)
    low = rest - middle
    row = lax.broadcasted_iota(jnp.int32, (16, width), 0)
    zero = jnp.zeros((16, width), f32)
    both = jnp.where(row == 0, high, jnp.where(row == 1, middle, jnp.where(row == 2, low, zero)))
    return both.astype(bf16)


def joined_rows(rows):
    rows = rows.astype(f32)
    return (rows[0:1] + rows[1:2]) + rows[2:3]


SUB = 2
DOCS = 16
PAD = 128 - HW


def ends_of(lengths):
    ends = [lengths[0]]
    for i in range(1, DOCS):
        ends.append(ends[-1] + lengths[i])
    return ends


def doc_of(place, ends):
    doc = (place >= ends[0]).astype(jnp.int32)
    for end in ends[1:]:
        doc = doc + (place >= end).astype(jnp.int32)
    return doc


def attend_kernel(lengths, q_ref, kv_ref, out_ref, k_s, q_s, m_s, l_s, acc_s):
    ends = ends_of(lengths)
    query_base = lax.axis_index("z") * (YS * QB)
    key_base = lax.axis_index("y") * KB
    mine = pl.ds(pl.multiple_of(lax.axis_index("c") * HW, HW), HW)
    row = lax.broadcasted_iota(jnp.int32, (YS, QB), 0)
    lane = lax.broadcasted_iota(jnp.int32, (YS, QB), 1)
    query_doc = doc_of(query_base + row * QB + lane, ends)
    key_doc = doc_of(key_base + row * (YS * QB) + lane, ends)
    index = lax.broadcasted_iota(jnp.int32, (PAD, QB), 0)
    for i in range(ZS * CS):
        half = slice((i % CS) * ROWS, (i % CS + 1) * ROWS)
        same = index[:, half] == key_doc[i // CS : i // CS + 1, half]
        part = jnp.where(same, 1.0, 0.0).astype(bf16)
        k_s[i * ROWS : (i + 1) * ROWS, :] = jnp.transpose(
            jnp.concatenate([kv_ref[i, :HW, :], part], axis=0)
        )
    for i in range(YS):
        q_s[i, :HW, :] = jnp.concatenate(
            [q_ref[2 * i, mine, :], q_ref[2 * i + 1, mine, :]], axis=1
        )
        other = (index != query_doc[i : i + 1]) & (index < DOCS)
        q_s[i, HW:, :] = jnp.where(other, NEG, 0.0).astype(bf16)
    m_s[...] = jnp.full(m_s.shape, START, f32)
    l_s[...] = jnp.zeros(l_s.shape, f32)
    acc_s[...] = jnp.zeros(acc_s.shape, f32)

    def block(t, j):
        keys = k_s[pl.ds(j * KB, KB), :]
        values = jnp.concatenate([kv_ref[2 * j, HW:, :], kv_ref[2 * j + 1, HW:, :]], axis=1)
        for s in range(SUB):
            at = t * SUB + s
            scores = jnp.dot(keys, q_s[at], preferred_element_type=f32)
            before = m_s[at]
            now = jnp.maximum(before, jnp.max(scores, axis=0, keepdims=True))
            weights = jnp.exp2((scores - now) * SCALE2)
            rescale = jnp.exp2((before - now) * SCALE2)
            m_s[at] = now
            l_s[at] = l_s[at] * rescale + jnp.sum(weights, axis=0, keepdims=True)
            acc_s[at] = acc_s[at] * rescale + jnp.dot(
                values, weights.astype(bf16), preferred_element_type=f32
            )

    def query_step(t, _):
        begin = query_base + t * (SUB * QB)
        first = doc_of(begin, ends)
        last = doc_of(begin + (SUB * QB - 1), ends)

        def key_step(j, _):
            start = key_base + j * (YS * QB)
            least = doc_of(start, ends)
            most = doc_of(start + (KB - 1), ends)

            @pl.when((least <= last) & (most >= first))
            def _():
                block(t, j)

            return 0

        return lax.fori_loop(0, ZS, key_step, 0)

    lax.fori_loop(0, YS // SUB, query_step, 0)
    for i in range(YS):
        total = l_s[i]
        some = total > 0.0
        safe = jnp.where(some, total, 1.0)
        logs = jnp.where(some, m_s[i] * SCALE + jnp.log(safe), NEG)
        out_ref[i, :VD, :] = (acc_s[i] / safe).astype(bf16)
        out_ref[i, VD:, :] = split_rows(logs, QB)


def combine_kernel(in_ref, out_ref):
    logs = [joined_rows(in_ref[i, VD:, :]) for i in range(YS)]
    top = logs[0]
    for v in logs[1:]:
        top = jnp.maximum(top, v)
    total = jnp.zeros((1, QB), f32)
    mixed = jnp.zeros((VD, QB), f32)
    for i in range(YS):
        w = jnp.exp(logs[i] - top)
        total = total + w
        mixed = mixed + w * in_ref[i, :VD, :].astype(f32)
    head = (mixed / total).astype(bf16)
    tail = split_rows(top + jnp.log(total), QB)
    for c in range(CS):
        for x in range(XS):
            out_ref[c * XS + x, :VD, :] = head[:, c * ROWS : (c + 1) * ROWS]
            out_ref[c * XS + x, VD:, :] = tail[:, c * ROWS : (c + 1) * ROWS]


def output_kernel(x_at, in_ref, gain_ref, weight_ref, out_ref, log_ref):
    heads = []
    for x in range(XS):
        for c in range(CS):
            heads.append(in_ref[c * XS + x, :VD, :].astype(f32))
    joined = jnp.concatenate(heads, axis=0)
    square = jnp.sum(joined * joined, axis=0, keepdims=True) * (1.0 / joined.shape[0])
    normed = (joined * lax.rsqrt(square + EPS) * gain_ref[...]).astype(bf16)
    out_ref[...] = lax.dot_general(
        normed, weight_ref[...], (((0,), (0,)), ((), ())), preferred_element_type=f32
    ).astype(bf16)
    for c in range(CS):
        log_ref[c : c + 1, :] = joined_rows(in_ref[c * XS + x_at[0], VD:, :])


def smem():
    return pl.BlockSpec(memory_space=pltpu.SMEM)


def vmem():
    return pl.BlockSpec(memory_space=pltpu.VMEM)


def call(kernel, out_shape, scalars, arrays, scratch=()):
    many = isinstance(out_shape, (tuple, list))
    return pl.pallas_call(
        kernel,
        out_shape=out_shape,
        in_specs=[smem()] * len(scalars) + [vmem()] * len(arrays),
        out_specs=[vmem() for _ in out_shape] if many else vmem(),
        scratch_shapes=list(scratch),
        compiler_params=pltpu.CompilerParams(vmem_limit_bytes=32 * 1024 * 1024),
    )(*scalars, *arrays)


def per_device(
    tokens,
    doc_lengths,
    query_down,
    latent_down,
    rope_down,
    query_latent_gain,
    latent_gain,
    query_up,
    key_up,
    value_up,
    query_gain,
    key_gain,
    output_gain,
    output_weight,
):
    z_at, y_at, c_at, x_at = (lax.axis_index(a) for a in ("z", "y", "c", "x"))
    query_latent = norm_rows(
        jnp.dot(tokens, query_down, preferred_element_type=f32), query_latent_gain
    ).astype(bf16)
    key_latent = norm_rows(
        jnp.dot(tokens, latent_down, preferred_element_type=f32), latent_gain
    ).astype(bf16)
    rope_key = jnp.dot(tokens, rope_down, preferred_element_type=f32).astype(bf16)
    rank_q, rank_k = query_latent.shape[1], key_latent.shape[1]
    every = spread(jnp.concatenate([query_latent, key_latent, rope_key], axis=1), ("x",))
    every = every.reshape(ROWS, -1)
    query_rows = every[:, :rank_q]
    latent_rows = every[:, rank_q : rank_q + rank_k]
    rope_rows = every[:, rank_q + rank_k :]

    offset = ((z_at * YS + y_at) * CS + c_at) * ROWS
    places = offset + jnp.arange(ROWS, dtype=jnp.int32)
    inverse = THETA ** (-jnp.arange(HALF, dtype=f32) / HALF)
    angles = places.astype(f32)[None, :] * inverse[:, None]
    cosine, sine = jnp.cos(angles), jnp.sin(angles)

    kv_out = call(
        kv_kernel,
        jax.ShapeDtypeStruct((ZS * CS, KV, ROWS), bf16),
        (),
        (latent_rows, rope_rows, key_up, value_up, key_gain[:, None], cosine, sine),
    )
    kv_all = lax.all_to_all(kv_out, ("z", "c"), split_axis=0, concat_axis=0, tiled=True)
    q_out = call(
        q_kernel,
        jax.ShapeDtypeStruct((CS * HW, ROWS), bf16),
        (),
        (query_rows, query_up, query_gain[:, None], cosine, sine),
    )
    q_all = lax.all_gather(q_out, ("y", "c"), axis=0)

    parts = call(
        attend_kernel,
        jax.ShapeDtypeStruct((YS, MSG, QB), bf16),
        (doc_lengths,),
        (q_all, kv_all),
        scratch=(
            pltpu.VMEM((ZS * KB, 128), bf16),
            pltpu.VMEM((YS, 128, QB), bf16),
            pltpu.VMEM((YS, 1, QB), f32),
            pltpu.VMEM((YS, 1, QB), f32),
            pltpu.VMEM((YS, VD, QB), f32),
        ),
    )
    parts = lax.all_to_all(parts, "y", split_axis=0, concat_axis=0, tiled=True)
    heads = call(combine_kernel, jax.ShapeDtypeStruct((CS * XS, MSG, ROWS), bf16), (), (parts,))
    heads = lax.all_to_all(heads, ("c", "x"), split_axis=0, concat_axis=0, tiled=True)
    layer_output, log_totals = call(
        output_kernel,
        (
            jax.ShapeDtypeStruct((ROWS, output_weight.shape[1]), bf16),
            jax.ShapeDtypeStruct((CS, ROWS), f32),
        ),
        (x_at.astype(jnp.int32).reshape(1),),
        (heads, output_gain[:, None], output_weight),
    )
    return (layer_output, log_totals)


def solution(mesh):
    fine = Mesh(mesh.devices.reshape(ZS, YS, CS, XS), ("z", "y", "c", "x"))
    sp = ("z", "y", "c")

    return jax.shard_map(
        per_device,
        mesh=fine,
        in_specs=(
            P((*sp, "x"), None),
            P(),
            P(),
            P(),
            P(),
            P(),
            P(),
            P(None, "x"),
            P(None, "x"),
            P(None, "x"),
            P(),
            P(),
            P(),
            P(None, "x"),
        ),
        out_specs=(P(sp, "x"), P("x", sp)),
        check_vma=False,
    )
```

```python
import math

import jax
import jax.numpy as jnp
from jax import lax
from jax.experimental import pallas as pl
from jax.experimental.pallas import tpu as pltpu
from jax.sharding import Mesh, PartitionSpec as P


NOPE = 64
ROPE = 32
VD = 64
HW = NOPE + ROPE
KV = HW + VD
HALF = ROPE // 2

EPS = 1e-06
THETA = 10000.0
NEG = -1e30
START = -1e29
ZS, YS, CS, XS = 8, 8, 2, 4
ROWS = 128
QB = 256
KB = 256
MSG = VD + 16
SCALE = HW ** (-0.5)
SCALE2 = SCALE * math.log2(math.e)

f32 = jnp.float32
bf16 = jnp.bfloat16


def norm_rows(matrix, scaling):
    mean_square = jnp.mean(matrix * matrix, axis=-1, keepdims=True)
    return matrix * lax.rsqrt(mean_square + EPS) * scaling


def spread(value, axes):
    count = 1
    for a in axes:
        count *= lax.axis_size(a)
    copies = jnp.broadcast_to(value, (count, *value.shape))
    return lax.all_to_all(copies, axes, split_axis=0, concat_axis=0, tiled=True)


def rotated(a, b, cosine, sine):
    return a * cosine - b * sine, b * cosine + a * sine


def kv_kernel(lat_ref, rope_ref, key_up_ref, value_up_ref, gain_ref, cos_ref, sin_ref, out_ref):
    lat = lat_ref[...]
    plain = lax.dot_general(
        key_up_ref[...], lat, (((0,), (1,)), ((), ())), preferred_element_type=f32
    )
    value = lax.dot_general(
        value_up_ref[...], lat, (((0,), (1,)), ((), ())), preferred_element_type=f32
    ).astype(bf16)
    shared = rope_ref[...].astype(f32)
    shared = jnp.transpose(jnp.concatenate([shared, jnp.zeros((ROWS, 128 - ROPE), f32)], axis=1))
    shared = shared[:ROPE]
    shared_square = jnp.sum(shared * shared, axis=0, keepdims=True)
    gain = gain_ref[...]
    cosine, sine = cos_ref[...], sin_ref[...]
    for c in range(CS):
        mine = plain[c * NOPE : (c + 1) * NOPE]
        square = (jnp.sum(mine * mine, axis=0, keepdims=True) + shared_square) * (1.0 / HW)
        scale = lax.rsqrt(square + EPS)
        top = mine * scale * gain[:NOPE]
        low = shared * scale * gain[NOPE:]
        a, b = rotated(low[:HALF], low[HALF:], cosine, sine)
        block = jnp.concatenate([top, a, b], axis=0).astype(bf16)
        for z in range(ZS):
            out_ref[z * CS + c, :HW, :] = block
            out_ref[z * CS + c, HW:, :] = value[c * VD : (c + 1) * VD]


def q_kernel(lat_ref, query_up_ref, gain_ref, cos_ref, sin_ref, out_ref):
    raw = lax.dot_general(
        query_up_ref[...], lat_ref[...], (((0,), (1,)), ((), ())), preferred_element_type=f32
    )
    gain = gain_ref[...]
    cosine, sine = cos_ref[...], sin_ref[...]
    for c in range(CS):
        mine = raw[c * HW : (c + 1) * HW]
        square = jnp.sum(mine * mine, axis=0, keepdims=True) * (1.0 / HW)
        mine = mine * lax.rsqrt(square + EPS) * gain
        a, b = rotated(mine[NOPE : NOPE + HALF], mine[NOPE + HALF :], cosine, sine)
        block = jnp.concatenate([mine[:NOPE], a, b], axis=0).astype(bf16)
        out_ref[c * HW : (c + 1) * HW, :] = block


def split_rows(value, width):
    high = value.astype(bf16).astype(f32)
    rest = value - high
    middle = rest.astype(bf16).astype(f32)
    low = rest - middle
    row = lax.broadcasted_iota(jnp.int32, (16, width), 0)
    zero = jnp.zeros((16, width), f32)
    both = jnp.where(row == 0, high, jnp.where(row == 1, middle, jnp.where(row == 2, low, zero)))
    return both.astype(bf16)


def joined_rows(rows):
    rows = rows.astype(f32)
    return (rows[0:1] + rows[1:2]) + rows[2:3]


DOCS = 16
SLAB = 16
PAD = 128 - HW


def ends_of(lengths):
    ends = [lengths[0]]
    for i in range(1, DOCS):
        ends.append(ends[-1] + lengths[i])
    return ends


def doc_of(place, ends):
    doc = (place >= ends[0]).astype(jnp.int32)
    for end in ends[1:]:
        doc = doc + (place >= end).astype(jnp.int32)
    return doc


def attend_kernel(lengths, q_ref, kv_ref, out_ref, k_s, q_s, m_s, l_s, acc_s):
    ends = ends_of(lengths)
    query_base = lax.axis_index("z") * (YS * QB)
    key_base = lax.axis_index("y") * KB
    mine = pl.ds(pl.multiple_of(lax.axis_index("c") * HW, HW), HW)
    row = lax.broadcasted_iota(jnp.int32, (YS, QB), 0)
    lane = lax.broadcasted_iota(jnp.int32, (YS, QB), 1)
    query_doc = doc_of(query_base + row * QB + lane, ends)
    key_doc = doc_of(key_base + row * (YS * QB) + lane, ends)
    index = lax.broadcasted_iota(jnp.int32, (PAD, QB), 0)
    for i in range(ZS * CS):
        half = slice((i % CS) * ROWS, (i % CS + 1) * ROWS)
        same = index[:, half] == key_doc[i // CS : i // CS + 1, half]
        part = jnp.where(same, 1.0, 0.0).astype(bf16)
        k_s[i * ROWS : (i + 1) * ROWS, :] = jnp.transpose(
            jnp.concatenate([kv_ref[i, :HW, :], part], axis=0)
        )
    for i in range(YS):
        q_s[i, :HW, :] = jnp.concatenate(
            [q_ref[2 * i, mine, :], q_ref[2 * i + 1, mine, :]], axis=1
        )
        other = (index != query_doc[i : i + 1]) & (index < DOCS)
        q_s[i, HW:, :] = jnp.where(other, NEG, 0.0).astype(bf16)
    m_s[...] = jnp.full(m_s.shape, START, f32)
    l_s[...] = jnp.zeros(l_s.shape, f32)
    acc_s[...] = jnp.zeros(acc_s.shape, f32)

    first = doc_of(query_base, ends)
    last = doc_of(query_base + (YS * QB - 1), ends)

    def key_step(j, _):
        start = key_base + j * (YS * QB)
        least = doc_of(start, ends)
        most = doc_of(start + (KB - 1), ends)

        @pl.when((least <= last) & (most >= first))
        def _():
            keys = k_s[pl.ds(pl.multiple_of(j * KB, KB), KB), :]
            values = jnp.concatenate([kv_ref[2 * j, HW:, :], kv_ref[2 * j + 1, HW:, :]], axis=1)
            ahead = jnp.dot(keys, q_s[0], preferred_element_type=f32)
            peak = jnp.max(ahead, axis=0, keepdims=True)
            waiting = None
            for at in range(YS):
                scores = ahead
                before = m_s[at]
                now = jnp.maximum(before, peak)
                rescale = jnp.exp2((before - now) * SCALE2)
                m_s[at] = now
                if at + 1 < YS:
                    ahead = jnp.dot(keys, q_s[at + 1], preferred_element_type=f32)
                    peaks = jnp.full((8, QB), START, f32)
                sums = jnp.zeros((8, QB), f32)
                pieces = []
                for r in range(0, KB, SLAB):
                    w = jnp.exp2((scores[r : r + SLAB] - now) * SCALE2)
                    for i in range(0, SLAB, 8):
                        sums = sums + w[i : i + 8]
                    pieces.append(w.astype(bf16))
                    if at + 1 < YS:
                        for i in range(r, r + SLAB, 8):
                            peaks = jnp.maximum(peaks, ahead[i : i + 8])
                if waiting is not None:
                    was, scaled, product = waiting
                    acc_s[was] = acc_s[was] * scaled + product
                product = jnp.dot(
                    values, jnp.concatenate(pieces, axis=0), preferred_element_type=f32
                )
                waiting = (at, rescale, product)
                l_s[at] = l_s[at] * rescale + jnp.sum(sums, axis=0, keepdims=True)
                if at + 1 < YS:
                    peak = jnp.max(peaks, axis=0, keepdims=True)
            was, scaled, product = waiting
            acc_s[was] = acc_s[was] * scaled + product

        return 0

    lax.fori_loop(0, ZS, key_step, 0)
    for i in range(YS):
        total = l_s[i]
        some = total > 0.0
        safe = jnp.where(some, total, 1.0)
        logs = jnp.where(some, m_s[i] * SCALE + jnp.log(safe), NEG)
        out_ref[i, :VD, :] = (acc_s[i] / safe).astype(bf16)
        out_ref[i, VD:, :] = split_rows(logs, QB)


def combine_kernel(in_ref, out_ref):
    logs = [joined_rows(in_ref[i, VD:, :]) for i in range(YS)]
    top = logs[0]
    for v in logs[1:]:
        top = jnp.maximum(top, v)
    total = jnp.zeros((1, QB), f32)
    mixed = jnp.zeros((VD, QB), f32)
    for i in range(YS):
        w = jnp.exp(logs[i] - top)
        total = total + w
        mixed = mixed + w * in_ref[i, :VD, :].astype(f32)
    head = (mixed / total).astype(bf16)
    tail = split_rows(top + jnp.log(total), QB)
    for c in range(CS):
        for x in range(XS):
            out_ref[c * XS + x, :VD, :] = head[:, c * ROWS : (c + 1) * ROWS]
            out_ref[c * XS + x, VD:, :] = tail[:, c * ROWS : (c + 1) * ROWS]


def output_kernel(x_at, in_ref, gain_ref, weight_ref, out_ref, log_ref):
    heads = []
    for x in range(XS):
        for c in range(CS):
            heads.append(in_ref[c * XS + x, :VD, :].astype(f32))
    joined = jnp.concatenate(heads, axis=0)
    square = jnp.sum(joined * joined, axis=0, keepdims=True) * (1.0 / joined.shape[0])
    normed = (joined * lax.rsqrt(square + EPS) * gain_ref[...]).astype(bf16)
    out_ref[...] = lax.dot_general(
        normed, weight_ref[...], (((0,), (0,)), ((), ())), preferred_element_type=f32
    ).astype(bf16)
    for c in range(CS):
        log_ref[c : c + 1, :] = joined_rows(in_ref[c * XS + x_at[0], VD:, :])


def smem():
    return pl.BlockSpec(memory_space=pltpu.SMEM)


def vmem():
    return pl.BlockSpec(memory_space=pltpu.VMEM)


def call(kernel, out_shape, scalars, arrays, scratch=()):
    many = isinstance(out_shape, (tuple, list))
    return pl.pallas_call(
        kernel,
        out_shape=out_shape,
        in_specs=[smem()] * len(scalars) + [vmem()] * len(arrays),
        out_specs=[vmem() for _ in out_shape] if many else vmem(),
        scratch_shapes=list(scratch),
        compiler_params=pltpu.CompilerParams(vmem_limit_bytes=32 * 1024 * 1024),
    )(*scalars, *arrays)


def per_device(
    tokens,
    doc_lengths,
    query_down,
    latent_down,
    rope_down,
    query_latent_gain,
    latent_gain,
    query_up,
    key_up,
    value_up,
    query_gain,
    key_gain,
    output_gain,
    output_weight,
):
    z_at, y_at, c_at, x_at = (lax.axis_index(a) for a in ("z", "y", "c", "x"))
    query_latent = norm_rows(
        jnp.dot(tokens, query_down, preferred_element_type=f32), query_latent_gain
    ).astype(bf16)
    key_latent = norm_rows(
        jnp.dot(tokens, latent_down, preferred_element_type=f32), latent_gain
    ).astype(bf16)
    rope_key = jnp.dot(tokens, rope_down, preferred_element_type=f32).astype(bf16)
    rank_q, rank_k = query_latent.shape[1], key_latent.shape[1]
    every = spread(jnp.concatenate([query_latent, key_latent, rope_key], axis=1), ("x",))
    every = every.reshape(ROWS, -1)
    query_rows = every[:, :rank_q]
    latent_rows = every[:, rank_q : rank_q + rank_k]
    rope_rows = every[:, rank_q + rank_k :]

    offset = ((z_at * YS + y_at) * CS + c_at) * ROWS
    places = offset + jnp.arange(ROWS, dtype=jnp.int32)
    inverse = THETA ** (-jnp.arange(HALF, dtype=f32) / HALF)
    angles = places.astype(f32)[None, :] * inverse[:, None]
    cosine, sine = jnp.cos(angles), jnp.sin(angles)

    kv_out = call(
        kv_kernel,
        jax.ShapeDtypeStruct((ZS * CS, KV, ROWS), bf16),
        (),
        (latent_rows, rope_rows, key_up, value_up, key_gain[:, None], cosine, sine),
    )
    kv_all = lax.all_to_all(kv_out, ("z", "c"), split_axis=0, concat_axis=0, tiled=True)
    q_out = call(
        q_kernel,
        jax.ShapeDtypeStruct((CS * HW, ROWS), bf16),
        (),
        (query_rows, query_up, query_gain[:, None], cosine, sine),
    )
    q_all = lax.all_gather(q_out, ("y", "c"), axis=0)

    parts = call(
        attend_kernel,
        jax.ShapeDtypeStruct((YS, MSG, QB), bf16),
        (doc_lengths,),
        (q_all, kv_all),
        scratch=(
            pltpu.VMEM((ZS * KB, 128), bf16),
            pltpu.VMEM((YS, 128, QB), bf16),
            pltpu.VMEM((YS, 1, QB), f32),
            pltpu.VMEM((YS, 1, QB), f32),
            pltpu.VMEM((YS, VD, QB), f32),
        ),
    )
    parts = lax.all_to_all(parts, "y", split_axis=0, concat_axis=0, tiled=True)
    heads = call(combine_kernel, jax.ShapeDtypeStruct((CS * XS, MSG, ROWS), bf16), (), (parts,))
    heads = lax.all_to_all(heads, ("c", "x"), split_axis=0, concat_axis=0, tiled=True)
    layer_output, log_totals = call(
        output_kernel,
        (
            jax.ShapeDtypeStruct((ROWS, output_weight.shape[1]), bf16),
            jax.ShapeDtypeStruct((CS, ROWS), f32),
        ),
        (x_at.astype(jnp.int32).reshape(1),),
        (heads, output_gain[:, None], output_weight),
    )
    return (layer_output, log_totals)


def solution(mesh):
    fine = Mesh(mesh.devices.reshape(ZS, YS, CS, XS), ("z", "y", "c", "x"))
    sp = ("z", "y", "c")

    return jax.shard_map(
        per_device,
        mesh=fine,
        in_specs=(
            P((*sp, "x"), None),
            P(),
            P(),
            P(),
            P(),
            P(),
            P(),
            P(None, "x"),
            P(None, "x"),
            P(None, "x"),
            P(),
            P(),
            P(),
            P(None, "x"),
        ),
        out_specs=(P(sp, "x"), P("x", sp)),
        check_vma=False,
    )
```

```python
import math

import jax
import jax.numpy as jnp
from jax import lax
from jax.experimental import pallas as pl
from jax.experimental.pallas import tpu as pltpu
from jax.sharding import Mesh, PartitionSpec as P


NOPE = 64
ROPE = 32
VD = 64
HW = NOPE + ROPE
KV = HW + VD
HALF = ROPE // 2

EPS = 1e-06
THETA = 10000.0
NEG = -1e30
START = -1e29
ZS, YS, CS, XS = 8, 8, 2, 4
ROWS = 128
MINE = 32
QBLOCKS = 4
KBLOCKS = 2
ROPE_AT = (QBLOCKS + KBLOCKS) * MINE
STEPS = 4
STEP = 512
QB = 256
KB = 256
TAIL = 8
MSG = VD + TAIL
SCALE = HW ** (-0.5)
SCALE2 = SCALE * math.log2(math.e)

f32 = jnp.float32
bf16 = jnp.bfloat16


def start_kernel(
    tok_hbm, query_hbm, latent_hbm, rope_hbm, query_gain_hbm, latent_gain_hbm, out_ref,
    tok_s, query_s, latent_s, rope_s, query_gain_s, latent_gain_s, sems, query_sem, latent_sem,
):
    def part(i):
        return pl.ds(i * STEP, STEP)

    tok_copy = pltpu.make_async_copy(tok_hbm, tok_s, sems.at[0])
    tok_copy.start()
    copies = []
    for i in range(STEPS):
        pair = (
            pltpu.make_async_copy(query_hbm.at[part(i)], query_s.at[part(i)], query_sem.at[i]),
            pltpu.make_async_copy(latent_hbm.at[part(i)], latent_s.at[part(i)], latent_sem.at[i]),
        )
        for copy in pair:
            copy.start()
        copies.append(pair)
    later = (
        pltpu.make_async_copy(rope_hbm, rope_s, sems.at[1]),
        pltpu.make_async_copy(query_gain_hbm, query_gain_s, sems.at[2]),
        pltpu.make_async_copy(latent_gain_hbm, latent_gain_s, sems.at[3]),
    )
    for copy in later:
        copy.start()
    tok_copy.wait()
    query, latent = None, None
    for i in range(STEPS):
        for copy in copies[i]:
            copy.wait()
        tok = tok_s[:, i * STEP : (i + 1) * STEP]
        q = jnp.dot(tok, query_s[i * STEP : (i + 1) * STEP, :], preferred_element_type=f32)
        k = jnp.dot(tok, latent_s[i * STEP : (i + 1) * STEP, :], preferred_element_type=f32)
        query = q if query is None else query + q
        latent = k if latent is None else latent + k

    for copy in later:
        copy.wait()
    rope = lax.dot_general(
        tok_s[...], rope_s[...], (((1,), (1,)), ((), ())), preferred_element_type=f32
    )

    def normed(value, gain):
        square = jnp.sum(value * value, axis=1, keepdims=True) * (1.0 / value.shape[1])
        return (value * lax.rsqrt(square + EPS) * gain).astype(bf16)

    query = normed(query, query_gain_s[...])
    latent = normed(latent, latent_gain_s[...])
    rope = jnp.concatenate([rope[8 * g : 8 * g + 8] for g in range(MINE // 8)], axis=1)
    rope = rope.astype(bf16)
    for x in range(XS):
        for i in range(QBLOCKS):
            out_ref[x, i * MINE : (i + 1) * MINE, :] = query[:, i * 128 : (i + 1) * 128]
        for i in range(KBLOCKS):
            at = (QBLOCKS + i) * MINE
            out_ref[x, at : at + MINE, :] = latent[:, i * 128 : (i + 1) * 128]
        out_ref[x, ROPE_AT:, :] = rope


def rotated(a, b, cosine, sine):
    return a * cosine - b * sine, b * cosine + a * sine


def proj_kernel(
    in_ref, key_up_ref, value_up_ref, query_up_ref, key_gain_ref, query_gain_ref, cos_ref, sin_ref,
    kv_ref, q_ref,
):
    def rows(first, count):
        return jnp.concatenate(
            [
                jnp.concatenate(
                    [
                        in_ref[x, (first + i) * MINE : (first + i + 1) * MINE, :]
                        for i in range(count)
                    ],
                    axis=1,
                )
                for x in range(XS)
            ],
            axis=0,
        )

    lat = rows(QBLOCKS, KBLOCKS)
    plain = lax.dot_general(
        key_up_ref[...], lat, (((0,), (1,)), ((), ())), preferred_element_type=f32
    )
    value = lax.dot_general(
        value_up_ref[...], lat, (((0,), (1,)), ((), ())), preferred_element_type=f32
    ).astype(bf16)
    raw = lax.dot_general(
        query_up_ref[...], rows(0, QBLOCKS), (((1,), (1,)), ((), ())), preferred_element_type=f32
    )
    shared = jnp.concatenate(
        [
            in_ref[x, ROPE_AT:, :].astype(f32)[:, g * ROPE : (g + 1) * ROPE]
            for x in range(XS)
            for g in range(MINE // 8)
        ],
        axis=0,
    )
    shared = jnp.transpose(jnp.concatenate([shared, jnp.zeros((ROWS, 128 - ROPE), f32)], axis=1))
    shared = shared[:ROPE]
    shared_square = jnp.sum(shared * shared, axis=0, keepdims=True)
    gain = key_gain_ref[...]
    query_gain = query_gain_ref[...]
    cosine, sine = cos_ref[...], sin_ref[...]
    for c in range(CS):
        mine = plain[c * NOPE : (c + 1) * NOPE]
        square = (jnp.sum(mine * mine, axis=0, keepdims=True) + shared_square) * (1.0 / HW)
        scale = lax.rsqrt(square + EPS)
        top = mine * scale * gain[:NOPE]
        low = shared * scale * gain[NOPE:]
        a, b = rotated(low[:HALF], low[HALF:], cosine, sine)
        block = jnp.concatenate([top, a, b], axis=0).astype(bf16)
        for z in range(ZS):
            kv_ref[z * CS + c, :HW, :] = block
            kv_ref[z * CS + c, HW:, :] = value[c * VD : (c + 1) * VD]
    for c in range(CS):
        mine = raw[c * HW : (c + 1) * HW]
        square = jnp.sum(mine * mine, axis=0, keepdims=True) * (1.0 / HW)
        mine = mine * lax.rsqrt(square + EPS) * query_gain
        a, b = rotated(mine[NOPE : NOPE + HALF], mine[NOPE + HALF :], cosine, sine)
        q_ref[c * HW : (c + 1) * HW, :] = jnp.concatenate([mine[:NOPE], a, b], axis=0).astype(bf16)


def split_rows(value, width):
    high = value.astype(bf16).astype(f32)
    rest = value - high
    middle = rest.astype(bf16).astype(f32)
    low = rest - middle
    row = lax.broadcasted_iota(jnp.int32, (TAIL, width), 0)
    zero = jnp.zeros((TAIL, width), f32)
    both = jnp.where(row == 0, high, jnp.where(row == 1, middle, jnp.where(row == 2, low, zero)))
    return both.astype(bf16)


def joined_rows(rows):
    rows = rows.astype(f32)
    return (rows[0:1] + rows[1:2]) + rows[2:3]


DOCS = 16
SLAB = 16
AHEAD = 8
PAD = 128 - HW


def ends_of(lengths):
    ends = [lengths[0]]
    for i in range(1, DOCS):
        ends.append(ends[-1] + lengths[i])
    return ends


def doc_of(place, ends):
    doc = (place >= ends[0]).astype(jnp.int32)
    for end in ends[1:]:
        doc = doc + (place >= end).astype(jnp.int32)
    return doc


def attend_kernel(lengths, q_ref, kv_ref, out_ref, k_s, q_s, m_s, l_s, acc_s):
    ends = ends_of(lengths)
    query_base = lax.axis_index("z") * (YS * QB)
    key_base = lax.axis_index("y") * KB
    mine = pl.ds(pl.multiple_of(lax.axis_index("c") * HW, HW), HW)
    row = lax.broadcasted_iota(jnp.int32, (YS, QB), 0)
    lane = lax.broadcasted_iota(jnp.int32, (YS, QB), 1)
    query_doc = doc_of(query_base + row * QB + lane, ends)
    key_doc = doc_of(key_base + row * (YS * QB) + lane, ends)
    index = lax.broadcasted_iota(jnp.int32, (PAD, QB), 0)
    for i in range(ZS * CS):
        half = slice((i % CS) * ROWS, (i % CS + 1) * ROWS)
        same = index[:, half] == key_doc[i // CS : i // CS + 1, half]
        part = jnp.where(same, 1.0, 0.0).astype(bf16)
        k_s[i * ROWS : (i + 1) * ROWS, :] = jnp.transpose(
            jnp.concatenate([kv_ref[i, :HW, :], part], axis=0)
        )
    for i in range(YS):
        q_s[i, :HW, :] = jnp.concatenate(
            [q_ref[2 * i, mine, :], q_ref[2 * i + 1, mine, :]], axis=1
        )
        other = (index != query_doc[i : i + 1]) & (index < DOCS)
        q_s[i, HW:, :] = jnp.where(other, NEG, 0.0).astype(bf16)
    m_s[...] = jnp.full(m_s.shape, START, f32)
    l_s[...] = jnp.zeros(l_s.shape, f32)
    acc_s[...] = jnp.zeros(acc_s.shape, f32)

    first = doc_of(query_base, ends)
    last = doc_of(query_base + (YS * QB - 1), ends)

    def key_step(j, _):
        start = key_base + j * (YS * QB)
        least = doc_of(start, ends)
        most = doc_of(start + (KB - 1), ends)

        @pl.when((least <= last) & (most >= first))
        def _():
            keys = k_s[pl.ds(pl.multiple_of(j * KB, KB), KB), :]
            values = jnp.concatenate([kv_ref[2 * j, HW:, :], kv_ref[2 * j + 1, HW:, :]], axis=1)
            issued = [jnp.dot(keys, q_s[t], preferred_element_type=f32) for t in range(AHEAD)]
            peak = jnp.max(issued[0], axis=0, keepdims=True)
            waiting = None
            for at in range(YS):
                scores = issued[at]
                before = m_s[at]
                now = jnp.maximum(before, peak)
                rescale = jnp.exp2((before - now) * SCALE2)
                m_s[at] = now
                if at + AHEAD < YS:
                    issued.append(jnp.dot(keys, q_s[at + AHEAD], preferred_element_type=f32))
                if at + 1 < YS:
                    ahead = issued[at + 1]
                    peaks = jnp.full((8, QB), START, f32)
                sums = jnp.zeros((8, QB), f32)
                pieces = []
                for r in range(0, KB, SLAB):
                    w = jnp.exp2((scores[r : r + SLAB] - now) * SCALE2)
                    for i in range(0, SLAB, 8):
                        sums = sums + w[i : i + 8]
                    pieces.append(w.astype(bf16))
                    if at + 1 < YS:
                        for i in range(r, r + SLAB, 8):
                            peaks = jnp.maximum(peaks, ahead[i : i + 8])
                if waiting is not None:
                    was, scaled, product = waiting
                    acc_s[was] = acc_s[was] * scaled + product
                product = jnp.dot(
                    values, jnp.concatenate(pieces, axis=0), preferred_element_type=f32
                )
                waiting = (at, rescale, product)
                l_s[at] = l_s[at] * rescale + jnp.sum(sums, axis=0, keepdims=True)
                if at + 1 < YS:
                    peak = jnp.max(peaks, axis=0, keepdims=True)
            was, scaled, product = waiting
            acc_s[was] = acc_s[was] * scaled + product

        return 0

    lax.fori_loop(0, ZS, key_step, 0)
    for i in range(YS):
        total = l_s[i]
        some = total > 0.0
        safe = jnp.where(some, total, 1.0)
        logs = jnp.where(some, m_s[i] * SCALE + jnp.log(safe), NEG)
        out_ref[i, :VD, :] = (acc_s[i] / safe).astype(bf16)
        out_ref[i, VD:, :] = split_rows(logs, QB)


def combine_kernel(in_ref, out_ref):
    logs = [joined_rows(in_ref[i, VD:, :]) for i in range(YS)]
    top = logs[0]
    for v in logs[1:]:
        top = jnp.maximum(top, v)
    total = jnp.zeros((1, QB), f32)
    mixed = jnp.zeros((VD, QB), f32)
    for i in range(YS):
        w = jnp.exp(logs[i] - top)
        total = total + w
        mixed = mixed + w * in_ref[i, :VD, :].astype(f32)
    head = (mixed / total).astype(bf16)
    tail = split_rows(top + jnp.log(total), QB)
    for c in range(CS):
        for x in range(XS):
            out_ref[c * XS + x, :VD, :] = head[:, c * ROWS : (c + 1) * ROWS]
            out_ref[c * XS + x, VD:, :] = tail[:, c * ROWS : (c + 1) * ROWS]


def column_kernel(gain_ref, out_ref):
    gain = gain_ref[...]
    out_ref[...] = jnp.transpose(jnp.broadcast_to(gain, (ROWS, gain.shape[1])))


def output_kernel(x_at, in_ref, first_ref, second_ref, weight_ref, out_ref, log_ref):
    heads = []
    for x in range(XS):
        for c in range(CS):
            heads.append(in_ref[c * XS + x, :VD, :].astype(f32))
    joined = jnp.concatenate(heads, axis=0)
    square = jnp.sum(joined * joined, axis=0, keepdims=True) * (1.0 / joined.shape[0])
    gain = jnp.concatenate([first_ref[...], second_ref[...]], axis=0)
    normed = (joined * lax.rsqrt(square + EPS) * gain).astype(bf16)
    out_ref[...] = lax.dot_general(
        normed, weight_ref[...], (((0,), (0,)), ((), ())), preferred_element_type=f32
    ).astype(bf16)
    for c in range(CS):
        log_ref[c : c + 1, :] = joined_rows(in_ref[c * XS + x_at[0], VD:, :])


def smem():
    return pl.BlockSpec(memory_space=pltpu.SMEM)


def hbm():
    return pl.BlockSpec(memory_space=pltpu.HBM)


def vmem():
    return pl.BlockSpec(memory_space=pltpu.VMEM)


def call(kernel, out_shape, scalars, arrays, scratch=()):
    many = isinstance(out_shape, (tuple, list))
    return pl.pallas_call(
        kernel,
        out_shape=out_shape,
        in_specs=[smem()] * len(scalars) + [vmem()] * len(arrays),
        out_specs=[vmem() for _ in out_shape] if many else vmem(),
        scratch_shapes=list(scratch),
        compiler_params=pltpu.CompilerParams(vmem_limit_bytes=32 * 1024 * 1024),
    )(*scalars, *arrays)


def run_attend(doc_lengths, q_all, kv_all):
    return call(
        attend_kernel,
        jax.ShapeDtypeStruct((YS, MSG, QB), bf16),
        (doc_lengths,),
        (q_all, kv_all),
        scratch=(
            pltpu.VMEM((ZS * KB, 128), bf16),
            pltpu.VMEM((YS, 128, QB), bf16),
            pltpu.VMEM((YS, 1, QB), f32),
            pltpu.VMEM((YS, 1, QB), f32),
            pltpu.VMEM((YS, VD, QB), f32),
        ),
    )


def per_device(
    tokens,
    doc_lengths,
    query_down,
    latent_down,
    rope_down,
    query_latent_gain,
    latent_gain,
    query_up,
    key_up,
    value_up,
    query_gain,
    key_gain,
    output_gain,
    output_weight,
):
    z_at, y_at, c_at, x_at = (lax.axis_index(a) for a in ("z", "y", "c", "x"))
    packed = pl.pallas_call(
        start_kernel,
        out_shape=jax.ShapeDtypeStruct((XS, ROPE_AT + 8, 128), bf16),
        in_specs=[hbm()] * 6,
        out_specs=vmem(),
        scratch_shapes=[
            pltpu.VMEM(tokens.shape, bf16),
            pltpu.VMEM(query_down.shape, bf16),
            pltpu.VMEM(latent_down.shape, bf16),
            pltpu.VMEM(rope_down.shape[::-1], bf16),
            pltpu.VMEM((1, *query_latent_gain.shape), f32),
            pltpu.VMEM((1, *latent_gain.shape), f32),
            pltpu.SemaphoreType.DMA((4,)),
            pltpu.SemaphoreType.DMA((STEPS,)),
            pltpu.SemaphoreType.DMA((STEPS,)),
        ],
        compiler_params=pltpu.CompilerParams(vmem_limit_bytes=63 * 1024 * 1024),
        name="start",
    )(
        tokens,
        query_down,
        latent_down,
        rope_down.T,
        query_latent_gain.reshape(1, -1),
        latent_gain.reshape(1, -1),
    )
    every = lax.all_to_all(packed, "x", split_axis=0, concat_axis=0, tiled=True)

    offset = ((z_at * YS + y_at) * CS + c_at) * ROWS
    places = offset + jnp.arange(ROWS, dtype=jnp.int32)
    inverse = THETA ** (-jnp.arange(HALF, dtype=f32) / HALF)
    angles = places.astype(f32)[None, :] * inverse[:, None]
    cosine, sine = jnp.cos(angles), jnp.sin(angles)

    kv_out, q_out = call(
        proj_kernel,
        (
            jax.ShapeDtypeStruct((ZS * CS, KV, ROWS), bf16),
            jax.ShapeDtypeStruct((CS * HW, ROWS), bf16),
        ),
        (),
        (
            every,
            key_up,
            value_up,
            query_up.T,
            key_gain[:, None],
            query_gain[:, None],
            cosine,
            sine,
        ),
    )
    kv_all = lax.all_to_all(kv_out, ("z", "c"), split_axis=0, concat_axis=0, tiled=True)
    q_all = lax.all_gather(q_out, ("y", "c"), axis=0)

    parts = run_attend(doc_lengths, q_all, kv_all)
    parts = lax.all_to_all(parts, "y", split_axis=0, concat_axis=0, tiled=True)
    half = output_gain.shape[0] // 2
    column = jax.ShapeDtypeStruct((half, ROWS), f32)
    first = call(column_kernel, column, (), (output_gain[:half].reshape(1, -1),))
    second = call(column_kernel, column, (), (output_gain[half:].reshape(1, -1),))
    heads = call(combine_kernel, jax.ShapeDtypeStruct((CS * XS, MSG, ROWS), bf16), (), (parts,))
    heads = lax.all_to_all(heads, ("c", "x"), split_axis=0, concat_axis=0, tiled=True)
    layer_output, log_totals = call(
        output_kernel,
        (
            jax.ShapeDtypeStruct((ROWS, output_weight.shape[1]), bf16),
            jax.ShapeDtypeStruct((CS, ROWS), f32),
        ),
        (x_at.astype(jnp.int32).reshape(1),),
        (heads, first, second, output_weight),
    )
    return (layer_output, log_totals)


def solution(mesh):
    fine = Mesh(mesh.devices.reshape(ZS, YS, CS, XS), ("z", "y", "c", "x"))
    sp = ("z", "y", "c")

    return jax.shard_map(
        per_device,
        mesh=fine,
        in_specs=(
            P((*sp, "x"), None),
            P(),
            P(),
            P(),
            P(),
            P(),
            P(),
            P(None, "x"),
            P(None, "x"),
            P(None, "x"),
            P(),
            P(),
            P(),
            P(None, "x"),
        ),
        out_specs=(P(sp, "x"), P("x", sp)),
        check_vma=False,
    )
```

```python
import math

import jax
import jax.numpy as jnp
from jax import lax
from jax.experimental import pallas as pl
from jax.experimental.pallas import tpu as pltpu
from jax.sharding import Mesh, PartitionSpec as P


NOPE = 64
ROPE = 32
VD = 64
HW = NOPE + ROPE
KV = HW + VD
HALF = ROPE // 2

EPS = 1e-06
THETA = 10000.0
NEG = -1e30
START = -1e29
ZS, YS, CS, XS = 8, 8, 2, 4
ROWS = 128
MINE = 32
QBLOCKS = 4
KBLOCKS = 2
ROPE_AT = (QBLOCKS + KBLOCKS) * MINE
STEPS = 4
STEP = 512
QB = 256
KB = 256
TAIL = 8
MSG = VD + TAIL
SCALE = HW ** (-0.5)
SCALE2 = SCALE * math.log2(math.e)

f32 = jnp.float32
bf16 = jnp.bfloat16


def start_kernel(
    tok_hbm, query_hbm, latent_hbm, rope_hbm, query_gain_hbm, latent_gain_hbm, out_hbm,
    tok_s, query_s, latent_s, rope_s, query_gain_s, latent_gain_s, out_s,
    sems, query_sem, latent_sem, out_sem,
):
    def part(i):
        return pl.ds(i * STEP, STEP)

    tok_copy = pltpu.make_async_copy(tok_hbm, tok_s, sems.at[0])
    tok_copy.start()
    later = (
        pltpu.make_async_copy(rope_hbm, rope_s, sems.at[1]),
        pltpu.make_async_copy(query_gain_hbm, query_gain_s, sems.at[2]),
        pltpu.make_async_copy(latent_gain_hbm, latent_gain_s, sems.at[3]),
    )
    for copy in later:
        copy.start()
    copies = []
    for i in range(STEPS):
        pair = (
            pltpu.make_async_copy(query_hbm.at[part(i)], query_s.at[part(i)], query_sem.at[i]),
            pltpu.make_async_copy(latent_hbm.at[part(i)], latent_s.at[part(i)], latent_sem.at[i]),
        )
        for copy in pair:
            copy.start()
        copies.append(pair)
    tok_copy.wait()
    for copy in later:
        copy.wait()
    rope = lax.dot_general(
        tok_s[...], rope_s[...], (((1,), (1,)), ((), ())), preferred_element_type=f32
    )
    query, latent = None, None
    for i in range(STEPS):
        for copy in copies[i]:
            copy.wait()
        tok = tok_s[:, i * STEP : (i + 1) * STEP]
        q = jnp.dot(tok, query_s[i * STEP : (i + 1) * STEP, :], preferred_element_type=f32)
        k = jnp.dot(tok, latent_s[i * STEP : (i + 1) * STEP, :], preferred_element_type=f32)
        query = q if query is None else query + q
        latent = k if latent is None else latent + k


    def normed(value, gain):
        square = jnp.sum(value * value, axis=1, keepdims=True) * (1.0 / value.shape[1])
        return (value * lax.rsqrt(square + EPS) * gain).astype(bf16)

    query = normed(query, query_gain_s[...])
    latent = normed(latent, latent_gain_s[...])
    rope = jnp.concatenate([rope[8 * g : 8 * g + 8] for g in range(MINE // 8)], axis=1)
    rope = rope.astype(bf16)
    for i in range(QBLOCKS):
        out_s[i * MINE : (i + 1) * MINE, :] = query[:, i * 128 : (i + 1) * 128]
    for i in range(KBLOCKS):
        at = (QBLOCKS + i) * MINE
        out_s[at : at + MINE, :] = latent[:, i * 128 : (i + 1) * 128]
    out_s[ROPE_AT:, :] = rope
    copies = [pltpu.make_async_copy(out_s, out_hbm.at[x], out_sem.at[x]) for x in range(XS)]
    for copy in copies:
        copy.start()
    for copy in copies:
        copy.wait()


def rotated(a, b, cosine, sine):
    return a * cosine - b * sine, b * cosine + a * sine


def proj_kernel(
    in_ref, key_up_ref, value_up_ref, query_up_ref, key_gain_ref, query_gain_ref, cos_ref, sin_ref,
    kv_hbm, q_ref, kv_s, kv_sem,
):
    def rows(first, count):
        return jnp.concatenate(
            [
                jnp.concatenate(
                    [
                        in_ref[x, (first + i) * MINE : (first + i + 1) * MINE, :]
                        for i in range(count)
                    ],
                    axis=1,
                )
                for x in range(XS)
            ],
            axis=0,
        )

    lat = rows(QBLOCKS, KBLOCKS)
    plain = lax.dot_general(
        key_up_ref[...], lat, (((0,), (1,)), ((), ())), preferred_element_type=f32
    )
    value = lax.dot_general(
        value_up_ref[...], lat, (((0,), (1,)), ((), ())), preferred_element_type=f32
    ).astype(bf16)
    raw = lax.dot_general(
        query_up_ref[...], rows(0, QBLOCKS), (((1,), (1,)), ((), ())), preferred_element_type=f32
    )
    shared = jnp.concatenate(
        [
            in_ref[x, ROPE_AT:, :].astype(f32)[:, g * ROPE : (g + 1) * ROPE]
            for x in range(XS)
            for g in range(MINE // 8)
        ],
        axis=0,
    )
    shared = jnp.transpose(jnp.concatenate([shared, jnp.zeros((ROWS, 128 - ROPE), f32)], axis=1))
    shared = shared[:ROPE]
    shared_square = jnp.sum(shared * shared, axis=0, keepdims=True)
    gain = key_gain_ref[...]
    query_gain = query_gain_ref[...]
    cosine, sine = cos_ref[...], sin_ref[...]
    copies = []
    for c in range(CS):
        mine = plain[c * NOPE : (c + 1) * NOPE]
        square = (jnp.sum(mine * mine, axis=0, keepdims=True) + shared_square) * (1.0 / HW)
        scale = lax.rsqrt(square + EPS)
        top = mine * scale * gain[:NOPE]
        low = shared * scale * gain[NOPE:]
        a, b = rotated(low[:HALF], low[HALF:], cosine, sine)
        kv_s[c, :HW, :] = jnp.concatenate([top, a, b], axis=0).astype(bf16)
        kv_s[c, HW:, :] = value[c * VD : (c + 1) * VD]
        for z in range(ZS):
            at = z * CS + c
            copies.append(pltpu.make_async_copy(kv_s.at[c], kv_hbm.at[at], kv_sem.at[at]))
            copies[-1].start()
    for c in range(CS):
        mine = raw[c * HW : (c + 1) * HW]
        square = jnp.sum(mine * mine, axis=0, keepdims=True) * (1.0 / HW)
        mine = mine * lax.rsqrt(square + EPS) * query_gain
        a, b = rotated(mine[NOPE : NOPE + HALF], mine[NOPE + HALF :], cosine, sine)
        q_ref[c * HW : (c + 1) * HW, :] = jnp.concatenate([mine[:NOPE], a, b], axis=0).astype(bf16)
    for copy in copies:
        copy.wait()


def split_rows(value, width):
    high = value.astype(bf16).astype(f32)
    rest = value - high
    middle = rest.astype(bf16).astype(f32)
    low = rest - middle
    row = lax.broadcasted_iota(jnp.int32, (TAIL, width), 0)
    zero = jnp.zeros((TAIL, width), f32)
    both = jnp.where(row == 0, high, jnp.where(row == 1, middle, jnp.where(row == 2, low, zero)))
    return both.astype(bf16)


def joined_rows(rows):
    rows = rows.astype(f32)
    return (rows[0:1] + rows[1:2]) + rows[2:3]


DOCS = 16
SLAB = 16
AHEAD = 8
PAD = 128 - HW


def table_kernel(lengths, query_ref, key_ref):
    row = lax.broadcasted_iota(jnp.int32, (YS, QB), 0)
    lane = lax.broadcasted_iota(jnp.int32, (YS, QB), 1)
    query_place = lax.axis_index("z") * (YS * QB) + row * QB + lane
    key_place = lax.axis_index("y") * KB + row * (YS * QB) + lane
    end = jnp.int32(0)
    query_doc = jnp.zeros((YS, QB), jnp.int32)
    key_doc = jnp.zeros((YS, QB), jnp.int32)
    for i in range(DOCS):
        end = end + lengths[i]
        query_doc = query_doc + (query_place >= end).astype(jnp.int32)
        key_doc = key_doc + (key_place >= end).astype(jnp.int32)
    query_ref[...] = query_doc
    key_ref[...] = key_doc


def attend_kernel(
    lengths_ref, query_doc_ref, key_doc_ref, q_ref, kv_ref, out_ref,
    lengths, sem, k_s, q_s, m_s, l_s, acc_s,
):
    lengths_copy = pltpu.make_async_copy(lengths_ref, lengths, sem)
    lengths_copy.start()
    query_base = lax.axis_index("z") * (YS * QB)
    key_base = lax.axis_index("y") * KB
    index = lax.broadcasted_iota(jnp.int32, (PAD, QB), 0)
    mine = pl.ds(pl.multiple_of(lax.axis_index("c") * HW, HW), HW)
    for i in range(ZS * CS):
        half = slice((i % CS) * ROWS, (i % CS + 1) * ROWS)
        same = index[:, half] == key_doc_ref[i // CS : i // CS + 1, half]
        part = jnp.where(same, 1.0, 0.0).astype(bf16)
        k_s[i * ROWS : (i + 1) * ROWS, :] = jnp.transpose(
            jnp.concatenate([kv_ref[i, :HW, :], part], axis=0)
        )
    for i in range(YS):
        q_s[i, :HW, :] = jnp.concatenate(
            [q_ref[2 * i, mine, :], q_ref[2 * i + 1, mine, :]], axis=1
        )
        other = (index != query_doc_ref[i : i + 1, :]) & (index < DOCS)
        q_s[i, HW:, :] = jnp.where(other, NEG, 0.0).astype(bf16)
    m_s[...] = jnp.full(m_s.shape, START, f32)
    l_s[...] = jnp.zeros(l_s.shape, f32)
    acc_s[...] = jnp.zeros(acc_s.shape, f32)

    lengths_copy.wait()
    end = jnp.int32(0)
    low, high = jnp.int32(0), jnp.int32(1 << 30)
    for i in range(DOCS):
        end = end + lengths[i]
        low = jnp.where(end <= query_base, end, low)
        high = jnp.minimum(high, jnp.where(end >= query_base + YS * QB, end, 1 << 30))

    def key_step(j, _):
        start = key_base + j * (YS * QB)

        @pl.when((start < high) & (start + KB > low))
        def _():
            keys = k_s[pl.ds(pl.multiple_of(j * KB, KB), KB), :]
            values = jnp.concatenate([kv_ref[2 * j, HW:, :], kv_ref[2 * j + 1, HW:, :]], axis=1)
            issued = [jnp.dot(keys, q_s[t], preferred_element_type=f32) for t in range(AHEAD)]
            peak = jnp.max(issued[0], axis=0, keepdims=True)
            waiting = None
            for at in range(YS):
                scores = issued[at]
                before = m_s[at]
                now = jnp.maximum(before, peak)
                rescale = jnp.exp2((before - now) * SCALE2)
                m_s[at] = now
                if at + AHEAD < YS:
                    issued.append(jnp.dot(keys, q_s[at + AHEAD], preferred_element_type=f32))
                if at + 1 < YS:
                    ahead = issued[at + 1]
                    peaks = jnp.full((8, QB), START, f32)
                sums = jnp.zeros((8, QB), f32)
                pieces = []
                for r in range(0, KB, SLAB):
                    w = jnp.exp2((scores[r : r + SLAB] - now) * SCALE2)
                    for i in range(0, SLAB, 8):
                        sums = sums + w[i : i + 8]
                    pieces.append(w.astype(bf16))
                    if at + 1 < YS:
                        for i in range(r, r + SLAB, 8):
                            peaks = jnp.maximum(peaks, ahead[i : i + 8])
                if waiting is not None:
                    was, scaled, product = waiting
                    acc_s[was] = acc_s[was] * scaled + product
                product = jnp.dot(
                    values, jnp.concatenate(pieces, axis=0), preferred_element_type=f32
                )
                waiting = (at, rescale, product)
                l_s[at] = l_s[at] * rescale + jnp.sum(sums, axis=0, keepdims=True)
                if at + 1 < YS:
                    peak = jnp.max(peaks, axis=0, keepdims=True)
            was, scaled, product = waiting
            acc_s[was] = acc_s[was] * scaled + product

        return 0

    lax.fori_loop(0, ZS, key_step, 0)
    for i in range(YS):
        total = l_s[i]
        some = total > 0.0
        safe = jnp.where(some, total, 1.0)
        logs = jnp.where(some, m_s[i] * SCALE + jnp.log(safe), NEG)
        out_ref[i, :VD, :] = (acc_s[i] / safe).astype(bf16)
        out_ref[i, VD:, :] = split_rows(logs, QB)


def combine_kernel(in_ref, out_hbm, out_s, out_sem):
    logs = [joined_rows(in_ref[i, VD:, :]) for i in range(YS)]
    top = logs[0]
    for v in logs[1:]:
        top = jnp.maximum(top, v)
    total = jnp.zeros((1, QB), f32)
    mixed = jnp.zeros((VD, QB), f32)
    for i in range(YS):
        w = jnp.exp(logs[i] - top)
        total = total + w
        mixed = mixed + w * in_ref[i, :VD, :].astype(f32)
    head = (mixed / total).astype(bf16)
    tail = split_rows(top + jnp.log(total), QB)
    copies = []
    for c in range(CS):
        out_s[c, :VD, :] = head[:, c * ROWS : (c + 1) * ROWS]
        out_s[c, VD:, :] = tail[:, c * ROWS : (c + 1) * ROWS]
        for x in range(XS):
            at = c * XS + x
            copies.append(pltpu.make_async_copy(out_s.at[c], out_hbm.at[at], out_sem.at[at]))
            copies[-1].start()
    for copy in copies:
        copy.wait()


def output_kernel(x_at, in_ref, gain_ref, weight_ref, out_ref, log_ref):
    heads = []
    for x in range(XS):
        for c in range(CS):
            heads.append(in_ref[c * XS + x, :VD, :].astype(f32))
    joined = jnp.concatenate(heads, axis=0)
    square = jnp.sum(joined * joined, axis=0, keepdims=True) * (1.0 / joined.shape[0])
    normed = (joined * lax.rsqrt(square + EPS) * gain_ref[...]).astype(bf16)
    out_ref[...] = lax.dot_general(
        normed, weight_ref[...], (((0,), (0,)), ((), ())), preferred_element_type=f32
    ).astype(bf16)
    for c in range(CS):
        log_ref[c : c + 1, :] = joined_rows(in_ref[c * XS + x_at[0], VD:, :])


def smem():
    return pl.BlockSpec(memory_space=pltpu.SMEM)


def hbm():
    return pl.BlockSpec(memory_space=pltpu.HBM)


def vmem():
    return pl.BlockSpec(memory_space=pltpu.VMEM)


def call(kernel, out_shape, scalars, arrays, scratch=(), spaces=None):
    many = isinstance(out_shape, (tuple, list))
    return pl.pallas_call(
        kernel,
        out_shape=out_shape,
        in_specs=[smem()] * len(scalars) + [vmem()] * len(arrays),
        out_specs=spaces or ([vmem() for _ in out_shape] if many else vmem()),
        scratch_shapes=list(scratch),
        compiler_params=pltpu.CompilerParams(vmem_limit_bytes=32 * 1024 * 1024),
    )(*scalars, *arrays)


def run_attend(doc_lengths, query_docs, key_docs, q_all, kv_all):
    return call(
        attend_kernel,
        jax.ShapeDtypeStruct((YS, MSG, QB), bf16),
        (),
        (doc_lengths, query_docs, key_docs, q_all, kv_all),
        scratch=(
            pltpu.SMEM((DOCS,), jnp.int32),
            pltpu.SemaphoreType.DMA(()),
            pltpu.VMEM((ZS * KB, 128), bf16),
            pltpu.VMEM((YS, 128, QB), bf16),
            pltpu.VMEM((YS, 1, QB), f32),
            pltpu.VMEM((YS, 1, QB), f32),
            pltpu.VMEM((YS, VD, QB), f32),
        ),
    )


def per_device(
    tokens,
    doc_lengths,
    query_down,
    latent_down,
    rope_down,
    query_latent_gain,
    latent_gain,
    query_up,
    key_up,
    value_up,
    query_gain,
    key_gain,
    output_gain,
    output_weight,
):
    z_at, y_at, c_at, x_at = (lax.axis_index(a) for a in ("z", "y", "c", "x"))
    packed = pl.pallas_call(
        start_kernel,
        out_shape=jax.ShapeDtypeStruct((XS, ROPE_AT + 8, 128), bf16),
        in_specs=[hbm()] * 6,
        out_specs=hbm(),
        scratch_shapes=[
            pltpu.VMEM(tokens.shape, bf16),
            pltpu.VMEM(query_down.shape, bf16),
            pltpu.VMEM(latent_down.shape, bf16),
            pltpu.VMEM(rope_down.shape[::-1], bf16),
            pltpu.VMEM((1, *query_latent_gain.shape), f32),
            pltpu.VMEM((1, *latent_gain.shape), f32),
            pltpu.VMEM((ROPE_AT + 8, 128), bf16),
            pltpu.SemaphoreType.DMA((4,)),
            pltpu.SemaphoreType.DMA((STEPS,)),
            pltpu.SemaphoreType.DMA((STEPS,)),
            pltpu.SemaphoreType.DMA((XS,)),
        ],
        compiler_params=pltpu.CompilerParams(vmem_limit_bytes=63 * 1024 * 1024),
        name="start",
    )(
        tokens,
        query_down,
        latent_down,
        rope_down.T,
        query_latent_gain.reshape(1, -1),
        latent_gain.reshape(1, -1),
    )
    every = lax.all_to_all(packed, "x", split_axis=0, concat_axis=0, tiled=True)

    offset = ((z_at * YS + y_at) * CS + c_at) * ROWS
    places = offset + jnp.arange(ROWS, dtype=jnp.int32)
    inverse = THETA ** (-jnp.arange(HALF, dtype=f32) / HALF)
    angles = places.astype(f32)[None, :] * inverse[:, None]
    cosine, sine = jnp.cos(angles), jnp.sin(angles)

    docs = jax.ShapeDtypeStruct((YS, QB), jnp.int32)
    query_docs, key_docs = call(table_kernel, (docs, docs), (doc_lengths,), ())
    kv_out, q_out = call(
        proj_kernel,
        (
            jax.ShapeDtypeStruct((ZS * CS, KV, ROWS), bf16),
            jax.ShapeDtypeStruct((CS * HW, ROWS), bf16),
        ),
        (),
        (
            every,
            key_up,
            value_up,
            query_up.T,
            key_gain[:, None],
            query_gain[:, None],
            cosine,
            sine,
        ),
        scratch=(pltpu.VMEM((CS, KV, ROWS), bf16), pltpu.SemaphoreType.DMA((ZS * CS,))),
        spaces=[hbm(), vmem()],
    )
    kv_all = lax.all_to_all(kv_out, ("z", "c"), split_axis=0, concat_axis=0, tiled=True)
    q_all = lax.all_gather(q_out, ("y", "c"), axis=0)

    parts = run_attend(doc_lengths, query_docs, key_docs, q_all, kv_all)
    parts = lax.all_to_all(parts, "y", split_axis=0, concat_axis=0, tiled=True)
    heads = call(
        combine_kernel,
        jax.ShapeDtypeStruct((CS * XS, MSG, ROWS), bf16),
        (),
        (parts,),
        scratch=(pltpu.VMEM((CS, MSG, ROWS), bf16), pltpu.SemaphoreType.DMA((CS * XS,))),
        spaces=hbm(),
    )
    heads = lax.all_to_all(heads, ("c", "x"), split_axis=0, concat_axis=0, tiled=True)
    layer_output, log_totals = call(
        output_kernel,
        (
            jax.ShapeDtypeStruct((ROWS, output_weight.shape[1]), bf16),
            jax.ShapeDtypeStruct((CS, ROWS), f32),
        ),
        (x_at.astype(jnp.int32).reshape(1),),
        (heads, output_gain[:, None], output_weight),
    )
    return (layer_output, log_totals)


def solution(mesh):
    fine = Mesh(mesh.devices.reshape(ZS, YS, CS, XS), ("z", "y", "c", "x"))
    sp = ("z", "y", "c")

    return jax.shard_map(
        per_device,
        mesh=fine,
        in_specs=(
            P((*sp, "x"), None),
            P(),
            P(),
            P(),
            P(),
            P(),
            P(),
            P(None, "x"),
            P(None, "x"),
            P(None, "x"),
            P(),
            P(),
            P(),
            P(None, "x"),
        ),
        out_specs=(P(sp, "x"), P("x", sp)),
        check_vma=False,
    )
```

```python
import math

import jax
import jax.numpy as jnp
from jax import lax
from jax.experimental import pallas as pl
from jax.experimental.pallas import tpu as pltpu
from jax.sharding import Mesh, PartitionSpec as P


NOPE = 64
ROPE = 32
VD = 64
HW = NOPE + ROPE
KV = HW + VD
HALF = ROPE // 2

EPS = 1e-06
THETA = 10000.0
NEG = -1e30
START = -1e29
ZS, YS, CS, XS = 8, 8, 2, 4
ROWS = 128
MINE = 32
QBLOCKS = 4
KBLOCKS = 2
ROPE_AT = (QBLOCKS + KBLOCKS) * MINE
STEPS = 4
STEP = 512
QB = 256
KB = 256
TAIL = 8
MSG = VD + TAIL
SCALE = HW ** (-0.5)
SCALE2 = SCALE * math.log2(math.e)

f32 = jnp.float32
bf16 = jnp.bfloat16


def start_kernel(
    tok_hbm, query_hbm, latent_hbm, rope_hbm, query_gain_hbm, latent_gain_hbm, out_ref,
    tok_s, query_s, latent_s, rope_s, query_gain_s, latent_gain_s, sems, query_sem, latent_sem,
):
    def part(i):
        return pl.ds(i * STEP, STEP)

    tok_copy = pltpu.make_async_copy(tok_hbm, tok_s, sems.at[0])
    tok_copy.start()
    copies = []
    for i in range(STEPS):
        pair = (
            pltpu.make_async_copy(query_hbm.at[part(i)], query_s.at[part(i)], query_sem.at[i]),
            pltpu.make_async_copy(latent_hbm.at[part(i)], latent_s.at[part(i)], latent_sem.at[i]),
        )
        for copy in pair:
            copy.start()
        copies.append(pair)
    later = (
        pltpu.make_async_copy(rope_hbm, rope_s, sems.at[1]),
        pltpu.make_async_copy(query_gain_hbm, query_gain_s, sems.at[2]),
        pltpu.make_async_copy(latent_gain_hbm, latent_gain_s, sems.at[3]),
    )
    for copy in later:
        copy.start()
    tok_copy.wait()
    query, latent = None, None
    for i in range(STEPS):
        for copy in copies[i]:
            copy.wait()
        tok = tok_s[:, i * STEP : (i + 1) * STEP]
        q = jnp.dot(tok, query_s[i * STEP : (i + 1) * STEP, :], preferred_element_type=f32)
        k = jnp.dot(tok, latent_s[i * STEP : (i + 1) * STEP, :], preferred_element_type=f32)
        query = q if query is None else query + q
        latent = k if latent is None else latent + k

    for copy in later:
        copy.wait()
    rope = lax.dot_general(
        tok_s[...], rope_s[...], (((1,), (1,)), ((), ())), preferred_element_type=f32
    )

    def normed(value, gain):
        square = jnp.sum(value * value, axis=1, keepdims=True) * (1.0 / value.shape[1])
        return (value * lax.rsqrt(square + EPS) * gain).astype(bf16)

    query = normed(query, query_gain_s[...])
    latent = normed(latent, latent_gain_s[...])
    rope = jnp.concatenate([rope[8 * g : 8 * g + 8] for g in range(MINE // 8)], axis=1)
    rope = rope.astype(bf16)
    for x in range(XS):
        for i in range(QBLOCKS):
            out_ref[x, i * MINE : (i + 1) * MINE, :] = query[:, i * 128 : (i + 1) * 128]
        for i in range(KBLOCKS):
            at = (QBLOCKS + i) * MINE
            out_ref[x, at : at + MINE, :] = latent[:, i * 128 : (i + 1) * 128]
        out_ref[x, ROPE_AT:, :] = rope


def rotated(a, b, cosine, sine):
    return a * cosine - b * sine, b * cosine + a * sine


def proj_kernel(
    in_ref, key_up_ref, value_up_ref, query_up_ref, key_gain_ref, query_gain_ref, cos_ref, sin_ref,
    kv_ref, q_ref,
):
    def rows(first, count):
        return jnp.concatenate(
            [
                jnp.concatenate(
                    [
                        in_ref[x, (first + i) * MINE : (first + i + 1) * MINE, :]
                        for i in range(count)
                    ],
                    axis=1,
                )
                for x in range(XS)
            ],
            axis=0,
        )

    lat = rows(QBLOCKS, KBLOCKS)
    plain = lax.dot_general(
        key_up_ref[...], lat, (((0,), (1,)), ((), ())), preferred_element_type=f32
    )
    value = lax.dot_general(
        value_up_ref[...], lat, (((0,), (1,)), ((), ())), preferred_element_type=f32
    ).astype(bf16)
    raw = lax.dot_general(
        query_up_ref[...], rows(0, QBLOCKS), (((1,), (1,)), ((), ())), preferred_element_type=f32
    )
    shared = jnp.concatenate(
        [
            in_ref[x, ROPE_AT:, :].astype(f32)[:, g * ROPE : (g + 1) * ROPE]
            for x in range(XS)
            for g in range(MINE // 8)
        ],
        axis=0,
    )
    shared = jnp.transpose(jnp.concatenate([shared, jnp.zeros((ROWS, 128 - ROPE), f32)], axis=1))
    shared = shared[:ROPE]
    shared_square = jnp.sum(shared * shared, axis=0, keepdims=True)
    gain = key_gain_ref[...]
    query_gain = query_gain_ref[...]
    cosine, sine = cos_ref[...], sin_ref[...]
    for c in range(CS):
        mine = plain[c * NOPE : (c + 1) * NOPE]
        square = (jnp.sum(mine * mine, axis=0, keepdims=True) + shared_square) * (1.0 / HW)
        scale = lax.rsqrt(square + EPS)
        top = mine * scale * gain[:NOPE]
        low = shared * scale * gain[NOPE:]
        a, b = rotated(low[:HALF], low[HALF:], cosine, sine)
        block = jnp.concatenate([top, a, b], axis=0).astype(bf16)
        for z in range(ZS):
            kv_ref[z * CS + c, :HW, :] = block
            kv_ref[z * CS + c, HW:, :] = value[c * VD : (c + 1) * VD]
    for c in range(CS):
        mine = raw[c * HW : (c + 1) * HW]
        square = jnp.sum(mine * mine, axis=0, keepdims=True) * (1.0 / HW)
        mine = mine * lax.rsqrt(square + EPS) * query_gain
        a, b = rotated(mine[NOPE : NOPE + HALF], mine[NOPE + HALF :], cosine, sine)
        q_ref[c * HW : (c + 1) * HW, :] = jnp.concatenate([mine[:NOPE], a, b], axis=0).astype(bf16)


def split_rows(value, width):
    high = value.astype(bf16).astype(f32)
    rest = value - high
    middle = rest.astype(bf16).astype(f32)
    low = rest - middle
    row = lax.broadcasted_iota(jnp.int32, (TAIL, width), 0)
    zero = jnp.zeros((TAIL, width), f32)
    both = jnp.where(row == 0, high, jnp.where(row == 1, middle, jnp.where(row == 2, low, zero)))
    return both.astype(bf16)


def joined_rows(rows):
    rows = rows.astype(f32)
    return (rows[0:1] + rows[1:2]) + rows[2:3]


DOCS = 16
SLAB = 16
AHEAD = 8
PAD = 128 - HW


def table_kernel(lengths, query_ref, key_ref):
    row = lax.broadcasted_iota(jnp.int32, (YS, QB), 0)
    lane = lax.broadcasted_iota(jnp.int32, (YS, QB), 1)
    query_place = lax.axis_index("z") * (YS * QB) + row * QB + lane
    key_place = lax.axis_index("y") * KB + row * (YS * QB) + lane
    end = jnp.int32(0)
    query_doc = jnp.zeros((YS, QB), jnp.int32)
    key_doc = jnp.zeros((YS, QB), jnp.int32)
    for i in range(DOCS):
        end = end + lengths[i]
        query_doc = query_doc + (query_place >= end).astype(jnp.int32)
        key_doc = key_doc + (key_place >= end).astype(jnp.int32)
    query_ref[...] = query_doc
    key_ref[...] = key_doc


def attend_kernel(
    lengths_ref, query_doc_ref, key_doc_ref, q_ref, kv_ref, out_ref,
    lengths, sem, k_s, q_s, m_s, l_s, acc_s,
):
    lengths_copy = pltpu.make_async_copy(lengths_ref, lengths, sem)
    lengths_copy.start()
    query_base = lax.axis_index("z") * (YS * QB)
    key_base = lax.axis_index("y") * KB
    index = lax.broadcasted_iota(jnp.int32, (PAD, QB), 0)
    mine = pl.ds(pl.multiple_of(lax.axis_index("c") * HW, HW), HW)
    for i in range(ZS * CS):
        half = slice((i % CS) * ROWS, (i % CS + 1) * ROWS)
        same = index[:, half] == key_doc_ref[i // CS : i // CS + 1, half]
        part = jnp.where(same, 1.0, 0.0).astype(bf16)
        k_s[i * ROWS : (i + 1) * ROWS, :] = jnp.transpose(
            jnp.concatenate([kv_ref[i, :HW, :], part], axis=0)
        )
    for i in range(YS):
        q_s[i, :HW, :] = jnp.concatenate(
            [q_ref[2 * i, mine, :], q_ref[2 * i + 1, mine, :]], axis=1
        )
        other = (index != query_doc_ref[i : i + 1, :]) & (index < DOCS)
        q_s[i, HW:, :] = jnp.where(other, NEG, 0.0).astype(bf16)
    m_s[...] = jnp.full(m_s.shape, START, f32)
    l_s[...] = jnp.zeros(l_s.shape, f32)
    acc_s[...] = jnp.zeros(acc_s.shape, f32)

    lengths_copy.wait()
    end = jnp.int32(0)
    low, high = jnp.int32(0), jnp.int32(1 << 30)
    for i in range(DOCS):
        end = end + lengths[i]
        low = jnp.where(end <= query_base, end, low)
        high = jnp.minimum(high, jnp.where(end >= query_base + YS * QB, end, 1 << 30))

    def key_step(j, _):
        start = key_base + j * (YS * QB)

        @pl.when((start < high) & (start + KB > low))
        def _():
            keys = k_s[pl.ds(pl.multiple_of(j * KB, KB), KB), :]
            values = jnp.concatenate([kv_ref[2 * j, HW:, :], kv_ref[2 * j + 1, HW:, :]], axis=1)
            issued = [jnp.dot(keys, q_s[t], preferred_element_type=f32) for t in range(AHEAD)]
            peak = jnp.max(issued[0], axis=0, keepdims=True)
            waiting = None
            for at in range(YS):
                scores = issued[at]
                before = m_s[at]
                now = jnp.maximum(before, peak)
                rescale = jnp.exp2((before - now) * SCALE2)
                m_s[at] = now
                if at + AHEAD < YS:
                    issued.append(jnp.dot(keys, q_s[at + AHEAD], preferred_element_type=f32))
                if at + 1 < YS:
                    ahead = issued[at + 1]
                    peaks = jnp.full((8, QB), START, f32)
                sums = jnp.zeros((8, QB), f32)
                pieces = []
                for r in range(0, KB, SLAB):
                    w = jnp.exp2((scores[r : r + SLAB] - now) * SCALE2)
                    for i in range(0, SLAB, 8):
                        sums = sums + w[i : i + 8]
                    pieces.append(w.astype(bf16))
                    if at + 1 < YS:
                        for i in range(r, r + SLAB, 8):
                            peaks = jnp.maximum(peaks, ahead[i : i + 8])
                if waiting is not None:
                    was, scaled, product = waiting
                    acc_s[was] = acc_s[was] * scaled + product
                product = jnp.dot(
                    values, jnp.concatenate(pieces, axis=0), preferred_element_type=f32
                )
                waiting = (at, rescale, product)
                l_s[at] = l_s[at] * rescale + jnp.sum(sums, axis=0, keepdims=True)
                if at + 1 < YS:
                    peak = jnp.max(peaks, axis=0, keepdims=True)
            was, scaled, product = waiting
            acc_s[was] = acc_s[was] * scaled + product

        return 0

    lax.fori_loop(0, ZS, key_step, 0)
    for i in range(YS):
        total = l_s[i]
        some = total > 0.0
        safe = jnp.where(some, total, 1.0)
        logs = jnp.where(some, m_s[i] * SCALE + jnp.log(safe), NEG)
        out_ref[i, :VD, :] = (acc_s[i] / safe).astype(bf16)
        out_ref[i, VD:, :] = split_rows(logs, QB)


def combine_kernel(in_ref, out_ref):
    logs = [joined_rows(in_ref[i, VD:, :]) for i in range(YS)]
    top = logs[0]
    for v in logs[1:]:
        top = jnp.maximum(top, v)
    total = jnp.zeros((1, QB), f32)
    mixed = jnp.zeros((VD, QB), f32)
    for i in range(YS):
        w = jnp.exp(logs[i] - top)
        total = total + w
        mixed = mixed + w * in_ref[i, :VD, :].astype(f32)
    head = (mixed / total).astype(bf16)
    tail = split_rows(top + jnp.log(total), QB)
    for c in range(CS):
        for x in range(XS):
            out_ref[c * XS + x, :VD, :] = head[:, c * ROWS : (c + 1) * ROWS]
            out_ref[c * XS + x, VD:, :] = tail[:, c * ROWS : (c + 1) * ROWS]


def output_kernel(x_at, in_ref, gain_ref, weight_ref, out_ref, log_ref):
    heads = []
    for x in range(XS):
        for c in range(CS):
            heads.append(in_ref[c * XS + x, :VD, :].astype(f32))
    joined = jnp.concatenate(heads, axis=0)
    square = jnp.sum(joined * joined, axis=0, keepdims=True) * (1.0 / joined.shape[0])
    normed = (joined * lax.rsqrt(square + EPS) * gain_ref[...]).astype(bf16)
    out_ref[...] = lax.dot_general(
        normed, weight_ref[...], (((0,), (0,)), ((), ())), preferred_element_type=f32
    ).astype(bf16)
    for c in range(CS):
        log_ref[c : c + 1, :] = joined_rows(in_ref[c * XS + x_at[0], VD:, :])


def smem():
    return pl.BlockSpec(memory_space=pltpu.SMEM)


def hbm():
    return pl.BlockSpec(memory_space=pltpu.HBM)


def vmem():
    return pl.BlockSpec(memory_space=pltpu.VMEM)


def call(kernel, out_shape, scalars, arrays, scratch=()):
    many = isinstance(out_shape, (tuple, list))
    return pl.pallas_call(
        kernel,
        out_shape=out_shape,
        in_specs=[smem()] * len(scalars) + [vmem()] * len(arrays),
        out_specs=[vmem() for _ in out_shape] if many else vmem(),
        scratch_shapes=list(scratch),
        compiler_params=pltpu.CompilerParams(vmem_limit_bytes=32 * 1024 * 1024),
    )(*scalars, *arrays)


def run_attend(doc_lengths, query_docs, key_docs, q_all, kv_all):
    return call(
        attend_kernel,
        jax.ShapeDtypeStruct((YS, MSG, QB), bf16),
        (),
        (doc_lengths, query_docs, key_docs, q_all, kv_all),
        scratch=(
            pltpu.SMEM((DOCS,), jnp.int32),
            pltpu.SemaphoreType.DMA(()),
            pltpu.VMEM((ZS * KB, 128), bf16),
            pltpu.VMEM((YS, 128, QB), bf16),
            pltpu.VMEM((YS, 1, QB), f32),
            pltpu.VMEM((YS, 1, QB), f32),
            pltpu.VMEM((YS, VD, QB), f32),
        ),
    )


def per_device(
    tokens,
    doc_lengths,
    query_down,
    latent_down,
    rope_down,
    query_latent_gain,
    latent_gain,
    query_up,
    key_up,
    value_up,
    query_gain,
    key_gain,
    output_gain,
    output_weight,
):
    z_at, y_at, c_at, x_at = (lax.axis_index(a) for a in ("z", "y", "c", "x"))
    packed = pl.pallas_call(
        start_kernel,
        out_shape=jax.ShapeDtypeStruct((XS, ROPE_AT + 8, 128), bf16),
        in_specs=[hbm()] * 6,
        out_specs=vmem(),
        scratch_shapes=[
            pltpu.VMEM(tokens.shape, bf16),
            pltpu.VMEM(query_down.shape, bf16),
            pltpu.VMEM(latent_down.shape, bf16),
            pltpu.VMEM(rope_down.shape[::-1], bf16),
            pltpu.VMEM((1, *query_latent_gain.shape), f32),
            pltpu.VMEM((1, *latent_gain.shape), f32),
            pltpu.SemaphoreType.DMA((4,)),
            pltpu.SemaphoreType.DMA((STEPS,)),
            pltpu.SemaphoreType.DMA((STEPS,)),
        ],
        compiler_params=pltpu.CompilerParams(vmem_limit_bytes=63 * 1024 * 1024),
        name="start",
    )(
        tokens,
        query_down,
        latent_down,
        rope_down.T,
        query_latent_gain.reshape(1, -1),
        latent_gain.reshape(1, -1),
    )
    every = lax.all_to_all(packed, "x", split_axis=0, concat_axis=0, tiled=True)

    offset = ((z_at * YS + y_at) * CS + c_at) * ROWS
    places = offset + jnp.arange(ROWS, dtype=jnp.int32)
    inverse = THETA ** (-jnp.arange(HALF, dtype=f32) / HALF)
    angles = places.astype(f32)[None, :] * inverse[:, None]
    cosine, sine = jnp.cos(angles), jnp.sin(angles)

    docs = jax.ShapeDtypeStruct((YS, QB), jnp.int32)
    query_docs, key_docs = call(table_kernel, (docs, docs), (doc_lengths,), ())
    kv_out, q_out = call(
        proj_kernel,
        (
            jax.ShapeDtypeStruct((ZS * CS, KV, ROWS), bf16),
            jax.ShapeDtypeStruct((CS * HW, ROWS), bf16),
        ),
        (),
        (
            every,
            key_up,
            value_up,
            query_up.T,
            key_gain[:, None],
            query_gain[:, None],
            cosine,
            sine,
        ),
    )
    kv_all = lax.all_to_all(kv_out, ("z", "c"), split_axis=0, concat_axis=0, tiled=True)
    q_all = lax.all_gather(q_out, ("y", "c"), axis=0)

    parts = run_attend(doc_lengths, query_docs, key_docs, q_all, kv_all)
    parts = lax.all_to_all(parts, "y", split_axis=0, concat_axis=0, tiled=True)
    heads = call(combine_kernel, jax.ShapeDtypeStruct((CS * XS, MSG, ROWS), bf16), (), (parts,))
    heads = lax.all_to_all(heads, ("c", "x"), split_axis=0, concat_axis=0, tiled=True)
    layer_output, log_totals = call(
        output_kernel,
        (
            jax.ShapeDtypeStruct((ROWS, output_weight.shape[1]), bf16),
            jax.ShapeDtypeStruct((CS, ROWS), f32),
        ),
        (x_at.astype(jnp.int32).reshape(1),),
        (heads, output_gain[:, None], output_weight),
    )
    return (layer_output, log_totals)


def solution(mesh):
    fine = Mesh(mesh.devices.reshape(ZS, YS, CS, XS), ("z", "y", "c", "x"))
    sp = ("z", "y", "c")

    return jax.shard_map(
        per_device,
        mesh=fine,
        in_specs=(
            P((*sp, "x"), None),
            P(),
            P(),
            P(),
            P(),
            P(),
            P(),
            P(None, "x"),
            P(None, "x"),
            P(None, "x"),
            P(),
            P(),
            P(),
            P(None, "x"),
        ),
        out_specs=(P(sp, "x"), P("x", sp)),
        check_vma=False,
    )
```
